512 devices in a mesh: sp: 32 (over z, x), dp: 16 (over y, core).
Axes of the slice: x: 4, y: 8, z: 8, core: 2. Of those that a mesh axis runs over, the one named last changes fastest.
Arguments:
- query_rows: bfloat16 [16, 4096, 2048], P('dp', 'sp'), may hold values from -6 to 6
- key_rows: bfloat16 [16, 4096, 2048], P('dp', 'sp'), may hold values from -6 to 6
- value_rows: bfloat16 [16, 4096, 2048], P('dp', 'sp'), may hold values from -6 to 6
- decay_low: bfloat16 [16, 4096, 128], P('dp', 'sp'), may hold values from -5 to 5
- rate_low: bfloat16 [16, 4096, 128], P('dp', 'sp'), may hold values from -4 to 4
- decay_up: bfloat16 [128, 2048], replicated, may hold values from -0.5 to 0.5
- rate_up: bfloat16 [128, 2048], replicated, may hold values from -0.5 to 0.5
- decay_base: float32 [2048], replicated, may hold values from -12 to -2
- norm_gain: float32 [2048], replicated, may hold values from 0.1 to 1.9
- out_weight: bfloat16 [2048, 2048], P(None, 'dp'), may hold values from -0.125 to 0.125
Outputs:
- layer_out: bfloat16 [16, 4096, 2048], P('dp', 'sp')
The draws below stay inside these ranges and needn't reach their ends.
All inputs are finite; a program needn't handle non-finite values.
Results may differ from the reference program's by a relative error of at most 0.005.
Values may be sent and summed in bfloat16 or wider, within the bound.
A program may use at most 128 MiB of HBM per device.

```python
import jax
import jax.numpy as jnp
from jax import lax

D = 2048
HEADS = 32
HEAD = 64
LOW = 128
TOK_DEV = 128
WIDTH = 2048
LENGTH = 4096
BATCH = 16


def draw_decay_low(key, part):
    noise = jnp.clip(jax.random.normal(jax.random.fold_in(key, 11), (BATCH, LENGTH, LOW), jnp.float32), -4.0, 4.0)
    offsets = jax.random.uniform(jax.random.fold_in(key, 12), (BATCH, LENGTH // TOK_DEV, 1), jnp.float32, minval=-1.0, maxval=1.0)
    total = noise + jnp.repeat(offsets, TOK_DEV, axis=1)
    return jnp.clip(total, -5.0, 5.0).astype(jnp.bfloat16)


def draw_decay_base(key, part):
    picks = jax.random.randint(jax.random.fold_in(key, 21), (HEADS, 1), 0, 16)
    quick = picks < 8
    slow_rate = jax.random.uniform(jax.random.fold_in(key, 22), (HEADS, HEAD), jnp.float32, minval=0.2, maxval=1.0) / LENGTH
    quick_rate = jax.random.uniform(jax.random.fold_in(key, 23), (HEADS, HEAD), jnp.float32, minval=0.01, maxval=0.033)
    chosen = jnp.where(quick, quick_rate, slow_rate)
    return jnp.clip(jnp.log(chosen) + 0.5, -12.0, -2.0).reshape(WIDTH).astype(jnp.float32)


def block_levels(key, extent, pieces, least, top_value):
    level = 1.0
    for dim, parts in pieces:
        heights = jax.random.uniform(jax.random.fold_in(jax.random.fold_in(key, 6), dim), (parts,), jnp.float32, least / len(pieces), top_value / len(pieces))
        level = level * jnp.repeat(jnp.exp(heights), extent[dim] // parts).reshape((-1,) + (1,) * (len(extent) - 1 - dim))
    return level


def gaussian(stream_key, dims, deviation, reach, cuts=(), held_as=jnp.bfloat16):
    values = deviation * jax.random.normal(stream_key, dims, jnp.float32)
    if cuts:
        values = values * block_levels(stream_key, dims, cuts, -0.22, 0.18)
    return jnp.clip(values, -reach, reach).astype(held_as)


def setup_inputs(seed: int = 0) -> dict:
    splits = jax.random.split(jax.random.key(seed), 11)
    query_rows = gaussian(splits[0], (BATCH, LENGTH, WIDTH), 1.0, 6.0, ((0, 16), (1, 32)))
    key_rows = gaussian(splits[1], (BATCH, LENGTH, WIDTH), 1.0, 6.0, ((0, 16), (1, 32)))
    value_rows = gaussian(splits[2], (BATCH, LENGTH, WIDTH), 1.0, 6.0, ((0, 16), (1, 32)))
    decay_low = draw_decay_low(jax.random.fold_in(splits[10], 71), 0)
    rate_low = gaussian(splits[4], (BATCH, LENGTH, LOW), 1.0, 4.0, ((0, 16), (1, 32)))
    decay_up = gaussian(splits[5], (LOW, WIDTH), LOW ** -0.5, 0.5)
    rate_up = gaussian(splits[6], (LOW, WIDTH), LOW ** -0.5, 0.5)
    decay_base = draw_decay_base(jax.random.fold_in(splits[10], 71), 0)
    norm_gain = jnp.clip(1.0 + 0.18 * jax.random.normal(splits[8], (WIDTH,), jnp.float32), 0.1, 1.9)
    out_weight = gaussian(splits[9], (WIDTH, D), WIDTH ** -0.5, 0.125, ((1, 16),))
    return {"query_rows": query_rows, "key_rows": key_rows, "value_rows": value_rows, "decay_low": decay_low, "rate_low": rate_low, "decay_up": decay_up, "rate_up": rate_up, "decay_base": decay_base, "norm_gain": norm_gain, "out_weight": out_weight}


HIGHEST = lax.Precision.HIGHEST

def reference(query_rows, key_rows, value_rows, decay_low, rate_low, decay_up, rate_up, decay_base, norm_gain, out_weight):
    heads = query_rows.shape[2] // HEAD

    def one_sequence(inputs):
        reads, keyed, valued, low_decay, low_rate = inputs
        positions = reads.shape[0]
        squashed = jnp.tanh(low_decay.astype(jnp.float32)).astype(jnp.bfloat16)
        decay_pre = (decay_base + jnp.dot(squashed, decay_up, preferred_element_type=jnp.float32)).astype(jnp.bfloat16)
        rate_pre = jnp.dot(low_rate, rate_up, preferred_element_type=jnp.float32).astype(jnp.bfloat16)
        log_decay = -jnp.exp(-jax.nn.softplus(-decay_pre.astype(jnp.float32)) - 0.5)
        rate = jax.nn.sigmoid(rate_pre.astype(jnp.float32))
        head_shape = (positions, heads, HEAD)
        query_heads = reads.astype(jnp.float32).reshape(head_shape)
        key_heads = keyed.astype(jnp.float32).reshape(head_shape)
        value_heads = valued.astype(jnp.float32).reshape(head_shape)
        decay_heads = jnp.exp(log_decay).reshape(head_shape)
        unit_keys = key_heads * lax.rsqrt(1.0 + lax.optimization_barrier(jnp.sum(key_heads * key_heads, axis=-1, keepdims=True)))
        erase = unit_keys * rate.reshape(head_shape)

        def advance(state, inputs_now):
            query_now, decay_now, key_now, value_now, unit_now, erase_now = inputs_now
            removed = jnp.einsum('hvk,hk->hv', state, unit_now, precision=HIGHEST)
            state = state * decay_now[:, None, :] - removed[:, :, None] * erase_now[:, None, :] + value_now[:, :, None] * key_now[:, None, :]
            return (state, jnp.einsum('hvk,hk->hv', state, query_now, precision=HIGHEST))
        initial = jnp.zeros((heads, HEAD, HEAD), jnp.float32)
        _, readout = lax.scan(advance, initial, (query_heads, decay_heads, key_heads, value_heads, unit_keys, erase))
        average = lax.optimization_barrier(jnp.mean(readout, axis=-1, keepdims=True))
        centred = readout - average
        variance = lax.optimization_barrier(jnp.mean(centred * centred, axis=-1, keepdims=True))
        normed = (centred * lax.rsqrt(variance + 1.0)).reshape(positions, heads * HEAD)
        mix = (normed * norm_gain).astype(jnp.bfloat16)
        return jnp.dot(mix, out_weight, preferred_element_type=jnp.float32).astype(jnp.bfloat16)
    return lax.map(one_sequence, (query_rows, key_rows, value_rows, decay_low, rate_low))
```

```python
import functools
import math

import jax
import jax.numpy as jnp
from jax import lax
from jax.experimental import pallas as pl
from jax.experimental.pallas import tpu as pltpu
from jax.sharding import PartitionSpec as P

HEAD = 64
PAIR = 2 * HEAD
QUAD = 2 * PAIR
XDIM = 4

F32 = jnp.float32
BF16 = jnp.bfloat16
MESH = pl.DeviceIdType.MESH


def mm(left, right):
    return lax.dot_general(left, right, (((1,), (0,)), ((), ())), preferred_element_type=F32)


def mm_nt(left, right):
    return lax.dot_general(left, right, (((1,), (1,)), ((), ())), preferred_element_type=F32)


def mm_tn(left, right):
    return lax.dot_general(left, right, (((0,), (0,)), ((), ())), preferred_element_type=F32)


def split(x):
    high = x.astype(BF16)
    return high, (x - high.astype(F32)).astype(BF16)


def iota(shape, dim):
    return lax.broadcasted_iota(jnp.int32, shape, dim)


def cat(parts, axis):
    return jnp.concatenate(parts, axis=axis)


def diag2(a, b):
    return cat([cat([a, jnp.zeros_like(b)], 1), cat([jnp.zeros_like(a), b], 1)], 0)


def swap_halves(x):
    return pltpu.roll(x.astype(F32), HEAD, 1).astype(x.dtype)


def low_half(shape):
    return lax.rem(iota(shape, 1), PAIR) < HEAD


def stack_pair(x):
    here = low_half(x.shape)
    zero = jnp.zeros_like(x)
    return cat([jnp.where(here, x, zero), jnp.where(here, zero, x)], 0)


def same_head_ones(width, scale):
    same = (iota((width, width), 0) // HEAD) == (iota((width, width), 1) // HEAD)
    return jnp.where(same, F32(scale), F32(0.0)).astype(BF16)


def put_split(refs, at, x):
    high, low = split(x)
    refs[0][:, at] = high
    refs[1][:, at] = low


def prepare(size, at, q_ref, k_ref, squashed, rate_low, dup_ref, rup_ref, base_ref, ops, decay_buf, pair):
    middle = size // 2
    upto = jnp.where(iota((size, size), 0) >= iota((size, size), 1), F32(1.0), F32(0.0)).astype(BF16)
    upto = cat([upto, upto], 1)
    decay_pre = (base_ref[:, at] + mm(squashed, dup_ref[:, at])).astype(BF16).astype(F32)
    rate_pre = mm(rate_low, rup_ref[:, at]).astype(BF16).astype(F32)
    log_decay = -math.exp(-0.5) / (1.0 + jnp.exp(-decay_pre))
    rate = 1.0 / (1.0 + jnp.exp(-rate_pre))
    running = mm(upto, cat(split(log_decay), 0))
    centre = running[middle : middle + 1]
    final = running[size - 1 :]
    ahead = jnp.exp(running - centre)
    before = jnp.exp(running - log_decay - centre)
    behind = jnp.exp(centre - running)
    at_centre = jnp.exp(centre)
    at_end = jnp.exp(final - centre)
    k = k_ref[:, at].astype(F32)
    q = q_ref[:, at].astype(F32)
    unit = k * lax.rsqrt(1.0 + mm(cat(split(k * k), 1), cat([same_head_ones(QUAD, 1.0)] * 2, 0)))
    erase_from = unit * before
    read_mid = q * ahead
    key_to = k * behind
    erase_to = -(unit * rate) * behind
    put_split(ops["from"], at, erase_from)
    put_split(ops["read"], at, read_mid)
    put_split(ops["key"], at, key_to)
    put_split(ops["erase"], at, erase_to)
    ops["from_start"][:, at] = erase_from * at_centre
    ops["read_start"][:, at] = read_mid * at_centre
    ops["key_end"][:, at] = (key_to * at_end).astype(BF16)
    ops["erase_end"][:, at] = (erase_to * at_end).astype(BF16)
    decays = jnp.exp(final)
    for i in range(2):
        here = decays[:, i * PAIR : (i + 1) * PAIR]
        decay_buf[2 * (pair + i)] = here
        decay_buf[2 * (pair + i) + 1] = pltpu.roll(here, HEAD, 1)


def by_head(x):
    return diag2(x[:, :PAIR], x[:, PAIR:])


def grids(size, left, ops, at, keep):
    high, low = (stack_pair(ref[:, at]) for ref in left)
    right = cat([ops["key"][0][:, at], ops["erase"][0][:, at]], 0)
    rest = cat([ops["key"][1][:, at], ops["erase"][1][:, at]], 0)
    grid = mm_nt(cat([high, low], 1), cat([right, right], 1)) + mm_nt(high, rest)
    part = lambda i, j: jnp.where(keep, grid[i * size : (i + 1) * size, j * size : (j + 1) * size], 0.0)
    return split(cat([part(0, 0), part(1, 0)], 1)), split(cat([part(0, 1), part(1, 1)], 1))


def inverses(splits, size):
    negs = [high for high, _ in splits]
    row = iota((size, PAIR * 2), 0)
    col = lax.rem(iota((size, PAIR * 2), 1), PAIR)
    eye = jnp.where(row == col, F32(1.0), F32(0.0)).astype(BF16)
    found = None
    block = 1
    while block < size:
        pick = (row // (2 * block) == col // (2 * block)) & (row // block != col // block) & (row > col)
        pieces = [jnp.where(pick, n, jnp.zeros_like(n)) for n in negs]
        if found is None:
            found = [eye + p for p in pieces]
        elif block < 16:
            right = [mm(p, by_head(x)).astype(BF16) for p, x in zip(pieces, found)]
            found = [x + mm(x, by_head(y)).astype(BF16) for x, y in zip(found, right)]
        else:
            starts = list(range(block, size, 2 * block))
            take = lambda m: cat([m[s : s + block] for s in starts], 0) if len(starts) > 1 else m[block:]
            right = [mm(take(p), by_head(x)).astype(BF16) for p, x in zip(pieces, found)]
            blank = jnp.zeros((block, 2 * PAIR), BF16)
            spread = lambda m: cat(
                [part for j in range(len(starts)) for part in (blank, m[j * block : (j + 1) * block])], 0)
            right = [spread(y) for y in right]
            step = [mm(take(x), by_head(y)).astype(BF16) for x, y in zip(found, right)]
            found = [x + spread(t) for x, t in zip(found, step)]
        block *= 2
    out = []
    for (high, low), x in zip(splits, found):
        residual = (eye - x).astype(F32) + (mm(high, by_head(x)) + mm(low, by_head(x)))
        out.append((x, mm(x, by_head(residual.astype(BF16))).astype(BF16)))
    return out


def low_part(x):
    return jnp.where(low_half(x.shape), x, jnp.zeros_like(x))


def high_part(x):
    return jnp.where(low_half(x.shape), jnp.zeros_like(x), x)


def transitions(size, ats, v_ref, ops, solved_bufs):
    strict = iota((size, size), 0) > iota((size, size), 1)
    negs, sides = [], []
    for at in ats:
        keys, neg = grids(size, ops["from"], ops, at, strict)
        negs.append(neg)
        v = v_ref[:, at]
        values = diag2(high_part(swap_halves(v)), high_part(v))
        carried = mm(keys[0], values) + mm(keys[1], values)
        base = ops["from_start"][:, at]
        lows = cat([low_part(base), low_part(swap_halves(base))], 1)
        sides.append(split(lows + carried))
    found = inverses(negs, size)
    messages = []
    for at, x, side in zip(ats, found, sides):
        solved = split(mm(x[0], by_head(side[0])) + mm(x[0], by_head(side[1])) + mm(x[1], by_head(side[0])))
        wide = pl.ds(pl.multiple_of(2 * at.start, QUAD), QUAD)
        solved_bufs[0][:, wide] = solved[0]
        solved_bufs[1][:, wide] = solved[1]
        v = v_ref[:, at]
        ends = cat([ops["erase_end"][:, at], ops["key_end"][:, at]], 0)
        values = cat([high_part(swap_halves(v)), high_part(v)], 1)
        made = mm_tn(ends, cat([solved[0], values], 0)).astype(BF16)
        messages.append((made[:HEAD, :PAIR], made[HEAD:, PAIR:]))
    return messages


def readouts(size, at, v_ref, ops, solved_bufs, local_bufs):
    within = iota((size, size), 0) >= iota((size, size), 1)
    keys, erases = grids(size, ops["read"], ops, at, within)
    left = [cat([e[:, :PAIR], k[:, :PAIR], e[:, PAIR:], k[:, PAIR:]], 1) for k, e in zip(keys, erases)]
    wide = pl.ds(pl.multiple_of(2 * at.start, QUAD), QUAD)
    solved = solved_bufs[0][:, wide]
    v = v_ref[:, at]
    right = diag2(cat([solved[:, :PAIR], high_part(swap_halves(v))], 0), cat([solved[:, PAIR:], high_part(v)], 0))
    base = ops["read_start"][:, at]
    lows = cat([low_part(base), low_part(swap_halves(base))], 1)
    taken = mm(left[0], right) + mm(left[1], right) + mm(erases[0], by_head(solved_bufs[1][:, wide]))
    put_split(local_bufs, wide, lows + taken)


def mixer_kernel(devices, ranks, batch,
                 q_ref, k_ref, v_ref, low_ref, rate_ref, dup_ref, rup_ref, base_ref, gain_ref, w_ref,
                 out_ref,
                 from_high, from_low, read_high, read_low, key_high, key_low, erase_high, erase_low,
                 key_end, erase_end, from_start, read_start,
                 solved_high, solved_low, local_high, local_low, mix_buf,
                 message_buf, decay_buf, arrive_buf, arrive_decay, back_buf, start_buf, weight_buf, chain_buf,
                 message_sem, decay_sem, back_sem, sent_sem, sent_decay_sem, sent_back_sem,
                 right_sem, left_sem, cross_sem, mate_sem, sent_ring_sem, sent_cross_sem, sent_mate_sem, own_sem):
    size, width = q_ref.shape
    pairs = width // PAIR
    ops = {"from": (from_high, from_low), "read": (read_high, read_low), "key": (key_high, key_low),
           "erase": (erase_high, erase_low), "key_end": key_end, "erase_end": erase_end,
           "from_start": from_start, "read_start": read_start}
    solved_bufs = (solved_high, solved_low)
    local_bufs = (local_high, local_low)
    me = lax.axis_index("sp")
    rank = lax.axis_index("dp")
    length = ranks // 2
    half_way = length // 2
    core = lax.rem(rank, 2)
    line = rank // 2
    along = lambda step: lax.rem(line + step + length, length)
    at_rank = lambda row: {"dp": row * 2 + core}
    mate = {"dp": rank + 1 - 2 * core}
    x = lax.rem(me, XDIM)
    across = lambda step: {"sp": me - x + lax.rem(x + step + XDIM, XDIM)}
    parity = lax.rem(x, 2)
    rows = width // 2
    quarter = rows // 2

    barrier = pltpu.get_barrier_semaphore()

    @pl.loop(1, devices)
    def _(j):
        pl.semaphore_signal(barrier, inc=1, device_id={"sp": lax.rem(me + j, devices)}, device_id_type=MESH)

    for target in (at_rank(along(1)), at_rank(along(-1)), mate):
        pl.semaphore_signal(barrier, inc=1, device_id=target, device_id_type=MESH)
    own = pltpu.make_async_copy(w_ref, weight_buf.at[rank], own_sem)
    own.start()

    squashed = jnp.tanh(low_ref[...].astype(F32)).astype(BF16)
    rate_low = rate_ref[...]

    def prepare_quads(quads):
        for i in quads:
            prepare(size, pl.ds(pl.multiple_of(i * QUAD, QUAD), QUAD), q_ref, k_ref, squashed, rate_low,
                    dup_ref, rup_ref, base_ref, ops, decay_buf, i * 2)

    @pl.loop(0, pairs // batch)
    def _(b):
        prepare_quads([b * (batch // 2) + i for i in range(batch // 2)])

    pl.semaphore_wait(barrier, devices - 1 + 3)
    own.wait()

    piece = lambda source, start, count: weight_buf.at[
        source * 2 + core, pl.ds(pl.multiple_of(start, quarter), count)]

    def remote(ref, sem_out, sem_in, target):
        return pltpu.make_async_remote_copy(
            src_ref=ref, dst_ref=ref, send_sem=sem_out, recv_sem=sem_in, device_id=target, device_id_type=MESH)

    def ring(step, way):
        sign = 1 if way == 0 else -1
        source = along(-sign * (step - 1))
        if step < half_way:
            ref = piece(source, parity * rows, rows)
        else:
            ref = piece(source, parity * rows + way * quarter, quarter)
        sems = right_sem if way == 0 else left_sem
        return remote(ref, sent_ring_sem.at[way, step - 1], sems.at[step - 1], at_rank(along(sign)))

    def ring_arrival(step, way):
        sign = 1 if way == 0 else -1
        source = along(-sign * step)
        if step < half_way:
            ref = piece(source, parity * rows, rows)
        else:
            ref = piece(source, parity * rows + way * quarter, quarter)
        sems = right_sem if way == 0 else left_sem
        return remote(ref, sent_ring_sem.at[way, step - 1], sems.at[step - 1], at_rank(along(sign)))

    def cross(offset, way):
        source = along(offset)
        ref = piece(source, parity * rows + way * quarter, quarter)
        index = (offset + length) % length
        return remote(ref, sent_cross_sem.at[way, index], cross_sem.at[way, index], across(1 if way == 0 else -1))

    def cross_arrival(offset, way):
        source = along(offset)
        ref = piece(source, (1 - parity) * rows + way * quarter, quarter)
        index = (offset + length) % length
        return remote(ref, sent_cross_sem.at[way, index], cross_sem.at[way, index], across(1 if way == 0 else -1))

    def to_mate(offset, which):
        source = along(offset)
        index = (offset + length) % length
        start = (parity if which == 0 else 1 - parity) * rows
        return remote(piece(source, start, rows), sent_mate_sem.at[which, index], mate_sem.at[which, index], mate)

    def from_mate(offset, which):
        index = (offset + length) % length
        start = (parity if which == 0 else 1 - parity) * rows
        ref = weight_buf.at[along(offset) * 2 + 1 - core, pl.ds(pl.multiple_of(start, quarter), rows)]
        return remote(ref, sent_mate_sem.at[which, index], mate_sem.at[which, index], mate)

    def offsets(step):
        return [half_way] if step == half_way else [-step, step]

    for way in range(2):
        ring(1, way).start()
    for which in range(2):
        to_mate(0, which).start()

    def serve_ring(step):
        for way in range(2):
            ring_arrival(step, way).wait_recv()
            if step < half_way:
                ring(step + 1, way).start()
        for offset in offsets(step):
            for way in range(2):
                cross(offset, way).start()
            to_mate(offset, 0).start()

    served = set()

    def serve_cross(step):
        served.add(step)
        for offset in offsets(step):
            for way in range(2):
                cross_arrival(offset, way).wait_recv()
            to_mate(offset, 1).start()

    def head_copy(head, sender, target):
        return pltpu.make_async_remote_copy(
            src_ref=message_buf.at[head], dst_ref=arrive_buf.at[sender], send_sem=sent_sem, recv_sem=message_sem,
            device_id=target, device_id_type=MESH)

    def decay_copy(head, sender, target):
        return pltpu.make_async_remote_copy(
            src_ref=decay_buf.at[head], dst_ref=arrive_decay.at[sender], send_sem=sent_decay_sem,
            recv_sem=decay_sem, device_id=target, device_id_type=MESH)

    @pl.loop(0, pairs // batch)
    def _(b):
        ats = [pl.ds(pl.multiple_of((b * batch + i) * PAIR, PAIR), PAIR) for i in range(batch)]
        messages = transitions(size, ats, v_ref, ops, solved_bufs)
        for i, (first, second) in enumerate(messages):
            message_buf[2 * (b * batch + i)] = first
            message_buf[2 * (b * batch + i) + 1] = second
        count = 2 * batch

        @pl.loop(0, count)
        def _(j):
            head = b * count + lax.rem(me + j, count)

            @pl.when(head != me)
            def _():
                head_copy(head, me, {"sp": head}).start()
                decay_copy(head, me, {"sp": head}).start()

    arrive_buf[me] = message_buf[me]
    arrive_decay[me] = decay_buf[me]
    serve_ring(1)

    @pl.loop(0, pairs // batch)
    def _(b):
        for i in range(batch):
            readouts(size, pl.ds(pl.multiple_of((b * batch + i) * PAIR, PAIR), PAIR), v_ref, ops, solved_bufs,
                     local_bufs)

    serve_cross(1)
    if half_way > 1:
        serve_ring(2)

    others = pl.ds(0, devices - 1)
    pltpu.make_async_copy(arrive_buf.at[others], arrive_buf.at[others], message_sem).wait()
    pltpu.make_async_copy(arrive_decay.at[others], arrive_decay.at[others], decay_sem).wait()

    def back_copy(chunk, head, target):
        return pltpu.make_async_remote_copy(
            src_ref=back_buf.at[chunk], dst_ref=start_buf.at[head], send_sem=sent_back_sem, recv_sem=back_sem.at[head],
            device_id=target, device_id_type=MESH)

    row = iota((HEAD, PAIR), 0)
    lane = iota((HEAD, PAIR), 1)
    marker = jnp.where(lane == row + HEAD, F32(1.0), F32(0.0)).astype(BF16)
    lower = lane < HEAD

    chain_buf[...] = jnp.zeros_like(chain_buf)

    @pl.loop(0, devices)
    def _(c):
        state = chain_buf[...]
        average = jnp.mean(state, axis=0, keepdims=True)
        centred = jnp.where(lower, state - average, 0.0)
        packed = centred[: HEAD // 2] + pltpu.roll(centred[HEAD // 2 :], HEAD, 1)
        back_buf[c] = packed.astype(BF16)

        @pl.when(c != me)
        def _():
            back_copy(c, me, {"sp": c}).start()

        message = arrive_buf[c]
        left = jnp.where(lower, state.astype(BF16), marker)
        moved = mm_nt(left, cat([message, jnp.zeros_like(message)], 0))
        chain_buf[...] = moved + state * arrive_decay[c]

    start_buf[me] = back_buf[me]

    if half_way > 1:
        serve_cross(2)
    for step in range(3, half_way + 1):
        serve_ring(step)
        if step < half_way:
            serve_cross(step)

    mean_ones = cat([same_head_ones(PAIR, 1.0 / HEAD)] * 2, 0)
    centring = jnp.where(lane == row + HEAD, F32(1.0 - 1.0 / HEAD), F32(-1.0 / HEAD)).astype(BF16)

    def finish_pair(p):
        at = pl.ds(pl.multiple_of(p * PAIR, PAIR), PAIR)
        wide = pl.ds(pl.multiple_of(p * QUAD, QUAD), QUAD)
        rights = []
        for i in range(2):
            head = 2 * p + i

            @pl.when(head != me)
            def _():
                back_copy(me, head, {"sp": me}).wait_recv()

            packed = start_buf[head]
            rights.append(jnp.where(lower, cat([packed, swap_halves(packed)], 0), centring))
        right = diag2(rights[0], rights[1])
        centred = mm_nt(local_high[:, wide], right) + mm_nt(local_low[:, wide], right)
        variance = mm(cat(split(centred * centred), 1), mean_ones)
        mix_buf[:, at] = (centred * lax.rsqrt(variance + 1.0) * gain_ref[:, at]).astype(BF16)

    @pl.loop(0, pairs // batch)
    def _(b):
        for i in range(batch):
            finish_pair(b * batch + i)

    def project(offset):
        at = along(offset)
        weight = cat([weight_buf[2 * at], weight_buf[2 * at + 1]], 1)
        out_ref[:, pl.ds(pl.multiple_of(at * QUAD, QUAD), QUAD)] = mm(mix_buf[...], weight).astype(BF16)

    for which in range(2):
        from_mate(0, which).wait_recv()
    project(0)
    for step in range(1, half_way + 1):
        if step not in served:
            serve_cross(step)
        for offset in offsets(step):
            for which in range(2):
                from_mate(offset, which).wait_recv()
            project(offset)

    pltpu.make_async_copy(message_buf.at[others], message_buf.at[others], sent_sem).wait()
    pltpu.make_async_copy(decay_buf.at[others], decay_buf.at[others], sent_decay_sem).wait()
    pltpu.make_async_copy(back_buf.at[others], back_buf.at[others], sent_back_sem).wait()
    for step in range(1, half_way + 1):
        for way in range(2):
            ring(step, way).wait_send()
        for offset in offsets(step):
            for way in range(2):
                cross(offset, way).wait_send()
            for which in range(2):
                to_mate(offset, which).wait_send()
    for which in range(2):
        to_mate(0, which).wait_send()


def per_device(devices, ranks, query_rows, key_rows, value_rows, decay_low, rate_low, decay_up, rate_up,
               decay_base, norm_gain, out_weight):
    size, width = query_rows.shape[1:]
    heads = width // HEAD
    batch = min(4, width // PAIR)
    length = ranks // 2
    half_way = length // 2
    vmem = pl.BlockSpec(memory_space=pltpu.VMEM)
    dma = pltpu.SemaphoreType.DMA
    wide = lambda lanes: pltpu.VMEM((size, lanes), BF16)
    out = pl.pallas_call(
        functools.partial(mixer_kernel, devices, ranks, batch),
        in_specs=[vmem] * 9 + [pl.BlockSpec(memory_space=pl.ANY)],
        out_specs=vmem,
        out_shape=jax.ShapeDtypeStruct((size, out_weight.shape[1] * ranks), BF16),
        scratch_shapes=[wide(width) for _ in range(10)] + [pltpu.VMEM((size, width), F32)] * 2
        + [wide(2 * width) for _ in range(4)] + [wide(width)] + [
            pltpu.VMEM((heads, HEAD, PAIR), BF16),
            pltpu.VMEM((heads, 1, PAIR), F32),
            pltpu.VMEM((devices, HEAD, PAIR), BF16),
            pltpu.VMEM((devices, 1, PAIR), F32),
            pltpu.VMEM((devices, HEAD // 2, PAIR), BF16),
            pltpu.VMEM((heads, HEAD // 2, PAIR), BF16),
            pltpu.VMEM((ranks,) + out_weight.shape, BF16),
            pltpu.VMEM((HEAD, PAIR), F32),
            dma, dma, dma((heads,)), dma, dma, dma,
            dma((half_way,)), dma((half_way,)), dma((2, length)), dma((2, length)),
            dma((2, half_way)), dma((2, length)), dma((2, length)), dma,
        ],
        compiler_params=pltpu.CompilerParams(
            collective_id=0, has_side_effects=True, vmem_limit_bytes=60 * 2**20),
        cost_estimate=pl.CostEstimate(flops=10**10, bytes_accessed=10**7, transcendentals=0),
        name="mixer",
    )(query_rows[0], key_rows[0], value_rows[0], decay_low[0], rate_low[0], decay_up, rate_up,
      decay_base[None], norm_gain[None], out_weight)
    return out[None]


def solution(mesh):
    in_specs = (
        P("dp", "sp", None),
        P("dp", "sp", None),
        P("dp", "sp", None),
        P("dp", "sp", None),
        P("dp", "sp", None),
        P(),
        P(),
        P(),
        P(),
        P(None, "dp"),
    )
    return jax.shard_map(
        functools.partial(per_device, mesh.shape["sp"], mesh.shape["dp"]),
        mesh=mesh, in_specs=in_specs, out_specs=P("dp", "sp", None), check_vma=False,
    )
```

```python
import functools
import math

import jax
import jax.numpy as jnp
from jax import lax
from jax.experimental import pallas as pl
from jax.experimental.pallas import tpu as pltpu
from jax.sharding import PartitionSpec as P

HEAD = 64
PAIR = 2 * HEAD
QUAD = 2 * PAIR
XDIM = 4

F32 = jnp.float32
BF16 = jnp.bfloat16
MESH = pl.DeviceIdType.MESH


def mm(left, right):
    return lax.dot_general(left, right, (((1,), (0,)), ((), ())), preferred_element_type=F32)


def mm_nt(left, right):
    return lax.dot_general(left, right, (((1,), (1,)), ((), ())), preferred_element_type=F32)


def mm_tn(left, right):
    return lax.dot_general(left, right, (((0,), (0,)), ((), ())), preferred_element_type=F32)


def split(x):
    high = x.astype(BF16)
    return high, (x - high.astype(F32)).astype(BF16)


def iota(shape, dim):
    return lax.broadcasted_iota(jnp.int32, shape, dim)


def cat(parts, axis):
    return jnp.concatenate(parts, axis=axis)


def diag2(a, b):
    return cat([cat([a, jnp.zeros_like(b)], 1), cat([jnp.zeros_like(a), b], 1)], 0)


def swap_halves(x):
    return pltpu.roll(x.astype(F32), HEAD, 1).astype(x.dtype)


def low_half(shape):
    return lax.rem(iota(shape, 1), PAIR) < HEAD


def stack_pair(x):
    here = low_half(x.shape)
    zero = jnp.zeros_like(x)
    return cat([jnp.where(here, x, zero), jnp.where(here, zero, x)], 0)


def same_head_ones(width, scale):
    same = (iota((width, width), 0) // HEAD) == (iota((width, width), 1) // HEAD)
    return jnp.where(same, F32(scale), F32(0.0)).astype(BF16)


def put_split(refs, at, x):
    high, low = split(x)
    refs[0][:, at] = high
    refs[1][:, at] = low


def prepare(size, at, q_ref, k_ref, squashed, rate_low, dup_ref, rup_ref, base_ref, ops, decay_buf, pair):
    middle = size // 2
    upto = jnp.where(iota((size, size), 0) >= iota((size, size), 1), F32(1.0), F32(0.0)).astype(BF16)
    upto = cat([upto, upto], 1)
    decay_pre = (base_ref[:, at] + mm(squashed, dup_ref[:, at])).astype(BF16).astype(F32)
    rate_pre = mm(rate_low, rup_ref[:, at]).astype(BF16).astype(F32)
    log_decay = -math.exp(-0.5) / (1.0 + jnp.exp(-decay_pre))
    rate = 1.0 / (1.0 + jnp.exp(-rate_pre))
    running = mm(upto, cat(split(log_decay), 0))
    centre = running[middle : middle + 1]
    final = running[size - 1 :]
    ahead = jnp.exp(running - centre)
    before = jnp.exp(running - log_decay - centre)
    behind = jnp.exp(centre - running)
    at_centre = jnp.exp(centre)
    at_end = jnp.exp(final - centre)
    k = k_ref[:, at].astype(F32)
    q = q_ref[:, at].astype(F32)
    unit = k * lax.rsqrt(1.0 + mm(cat(split(k * k), 1), cat([same_head_ones(QUAD, 1.0)] * 2, 0)))
    erase_from = unit * before
    read_mid = q * ahead
    key_to = k * behind
    erase_to = -(unit * rate) * behind
    put_split(ops["from"], at, erase_from)
    put_split(ops["read"], at, read_mid)
    put_split(ops["key"], at, key_to)
    put_split(ops["erase"], at, erase_to)
    ops["from_start"][:, at] = erase_from * at_centre
    ops["read_start"][:, at] = read_mid * at_centre
    ops["key_end"][:, at] = (key_to * at_end).astype(BF16)
    ops["erase_end"][:, at] = (erase_to * at_end).astype(BF16)
    decays = jnp.exp(final)
    for i in range(2):
        here = decays[:, i * PAIR : (i + 1) * PAIR]
        decay_buf[2 * (pair + i)] = here
        decay_buf[2 * (pair + i) + 1] = pltpu.roll(here, HEAD, 1)


def by_head(x):
    return diag2(x[:, :PAIR], x[:, PAIR:])


def grids(size, left, ops, at, keep):
    high, low = (stack_pair(ref[:, at]) for ref in left)
    right = cat([ops["key"][0][:, at], ops["erase"][0][:, at]], 0)
    rest = cat([ops["key"][1][:, at], ops["erase"][1][:, at]], 0)
    grid = mm_nt(cat([high, low], 1), cat([right, right], 1)) + mm_nt(high, rest)
    part = lambda i, j: jnp.where(keep, grid[i * size : (i + 1) * size, j * size : (j + 1) * size], 0.0)
    return split(cat([part(0, 0), part(1, 0)], 1)), split(cat([part(0, 1), part(1, 1)], 1))


def inverses(splits, size):
    negs = [high for high, _ in splits]
    row = iota((size, PAIR * 2), 0)
    col = lax.rem(iota((size, PAIR * 2), 1), PAIR)
    eye = jnp.where(row == col, F32(1.0), F32(0.0)).astype(BF16)
    found = None
    block = 1
    while block < size:
        pick = (row // (2 * block) == col // (2 * block)) & (row // block != col // block) & (row > col)
        pieces = [jnp.where(pick, n, jnp.zeros_like(n)) for n in negs]
        if found is None:
            found = [eye + p for p in pieces]
        elif block < 16:
            right = [mm(p, by_head(x)).astype(BF16) for p, x in zip(pieces, found)]
            found = [x + mm(x, by_head(y)).astype(BF16) for x, y in zip(found, right)]
        else:
            starts = list(range(block, size, 2 * block))
            take = lambda m: cat([m[s : s + block] for s in starts], 0) if len(starts) > 1 else m[block:]
            right = [mm(take(p), by_head(x)).astype(BF16) for p, x in zip(pieces, found)]
            blank = jnp.zeros((block, 2 * PAIR), BF16)
            spread = lambda m: cat(
                [part for j in range(len(starts)) for part in (blank, m[j * block : (j + 1) * block])], 0)
            right = [spread(y) for y in right]
            step = [mm(take(x), by_head(y)).astype(BF16) for x, y in zip(found, right)]
            found = [x + spread(t) for x, t in zip(found, step)]
        block *= 2
    out = []
    for (high, low), x in zip(splits, found):
        residual = (eye - x).astype(F32) + (mm(high, by_head(x)) + mm(low, by_head(x)))
        out.append((x, mm(x, by_head(residual.astype(BF16))).astype(BF16)))
    return out


def low_part(x):
    return jnp.where(low_half(x.shape), x, jnp.zeros_like(x))


def high_part(x):
    return jnp.where(low_half(x.shape), jnp.zeros_like(x), x)


def transitions(size, ats, v_ref, ops, solved_bufs):
    strict = iota((size, size), 0) > iota((size, size), 1)
    negs, sides = [], []
    for at in ats:
        keys, neg = grids(size, ops["from"], ops, at, strict)
        negs.append(neg)
        v = v_ref[:, at]
        values = diag2(high_part(swap_halves(v)), high_part(v))
        carried = mm(keys[0], values) + mm(keys[1], values)
        base = ops["from_start"][:, at]
        lows = cat([low_part(base), low_part(swap_halves(base))], 1)
        sides.append(split(lows + carried))
    found = inverses(negs, size)
    messages = []
    for at, x, side in zip(ats, found, sides):
        solved = split(mm(x[0], by_head(side[0])) + mm(x[0], by_head(side[1])) + mm(x[1], by_head(side[0])))
        wide = pl.ds(pl.multiple_of(2 * at.start, QUAD), QUAD)
        solved_bufs[0][:, wide] = solved[0]
        solved_bufs[1][:, wide] = solved[1]
        v = v_ref[:, at]
        ends = cat([ops["erase_end"][:, at], ops["key_end"][:, at]], 0)
        values = cat([high_part(swap_halves(v)), high_part(v)], 1)
        made = mm_tn(ends, cat([solved[0], values], 0)).astype(BF16)
        messages.append((made[:HEAD, :PAIR], made[HEAD:, PAIR:]))
    return messages


def readouts(size, at, v_ref, ops, solved_bufs, local_bufs):
    within = iota((size, size), 0) >= iota((size, size), 1)
    keys, erases = grids(size, ops["read"], ops, at, within)
    left = [cat([e[:, :PAIR], k[:, :PAIR], e[:, PAIR:], k[:, PAIR:]], 1) for k, e in zip(keys, erases)]
    wide = pl.ds(pl.multiple_of(2 * at.start, QUAD), QUAD)
    solved = solved_bufs[0][:, wide]
    v = v_ref[:, at]
    right = diag2(cat([solved[:, :PAIR], high_part(swap_halves(v))], 0), cat([solved[:, PAIR:], high_part(v)], 0))
    base = ops["read_start"][:, at]
    lows = cat([low_part(base), low_part(swap_halves(base))], 1)
    taken = mm(left[0], right) + mm(left[1], right) + mm(erases[0], by_head(solved_bufs[1][:, wide]))
    put_split(local_bufs, wide, lows + taken)


def mixer_kernel(devices, ranks, batch,
                 q_ref, k_ref, v_ref, low_ref, rate_ref, dup_ref, rup_ref, base_ref, gain_ref, w_ref,
                 out_ref,
                 from_high, from_low, read_high, read_low, key_high, key_low, erase_high, erase_low,
                 key_end, erase_end, from_start, read_start,
                 solved_high, solved_low, local_high, local_low, mix_buf,
                 message_buf, decay_buf, arrive_buf, arrive_decay, back_buf, start_buf, weight_buf,
                 message_sem, decay_sem, back_sem, sent_sem, sent_decay_sem, sent_back_sem,
                 right_sem, left_sem, cross_sem, mate_sem, sent_ring_sem, sent_cross_sem, sent_mate_sem, own_sem):
    size, width = q_ref.shape
    pairs = width // PAIR
    ops = {"from": (from_high, from_low), "read": (read_high, read_low), "key": (key_high, key_low),
           "erase": (erase_high, erase_low), "key_end": key_end, "erase_end": erase_end,
           "from_start": from_start, "read_start": read_start}
    solved_bufs = (solved_high, solved_low)
    local_bufs = (local_high, local_low)
    me = lax.axis_index("sp")
    rank = lax.axis_index("dp")
    length = ranks // 2
    half_way = length // 2
    core = lax.rem(rank, 2)
    line = rank // 2
    along = lambda step: lax.rem(line + step + length, length)
    at_rank = lambda row: {"dp": row * 2 + core}
    mate = {"dp": rank + 1 - 2 * core}
    x = lax.rem(me, XDIM)
    across = lambda step: {"sp": me - x + lax.rem(x + step + XDIM, XDIM)}
    parity = lax.rem(x, 2)
    rows = width // 2
    quarter = rows // 2

    planes = devices // XDIM
    plane = me // XDIM
    my_head = lax.rem(x + planes * XDIM - plane, XDIM) * planes + plane

    def keeper(head):
        place = lax.rem(head, planes)
        return place * XDIM + lax.rem(place + head // planes, XDIM)

    barrier = pltpu.get_barrier_semaphore()

    @pl.loop(1, devices)
    def _(j):
        pl.semaphore_signal(barrier, inc=1, device_id={"sp": lax.rem(me + j, devices)}, device_id_type=MESH)

    for target in (at_rank(along(1)), at_rank(along(-1)), mate):
        pl.semaphore_signal(barrier, inc=1, device_id=target, device_id_type=MESH)
    own = pltpu.make_async_copy(w_ref, weight_buf.at[rank], own_sem)
    own.start()

    squashed = jnp.tanh(low_ref[...].astype(F32)).astype(BF16)
    rate_low = rate_ref[...]

    def prepare_quads(quads):
        for i in quads:
            prepare(size, pl.ds(pl.multiple_of(i * QUAD, QUAD), QUAD), q_ref, k_ref, squashed, rate_low,
                    dup_ref, rup_ref, base_ref, ops, decay_buf, i * 2)

    @pl.loop(0, pairs // batch)
    def _(b):
        prepare_quads([b * (batch // 2) + i for i in range(batch // 2)])

    pl.semaphore_wait(barrier, devices - 1 + 3)
    own.wait()

    piece = lambda source, start, count: weight_buf.at[
        source * 2 + core, pl.ds(pl.multiple_of(start, quarter), count)]

    def remote(ref, sem_out, sem_in, target):
        return pltpu.make_async_remote_copy(
            src_ref=ref, dst_ref=ref, send_sem=sem_out, recv_sem=sem_in, device_id=target, device_id_type=MESH)

    def ring(step, way):
        sign = 1 if way == 0 else -1
        source = along(-sign * (step - 1))
        if step < half_way:
            ref = piece(source, parity * rows, rows)
        else:
            ref = piece(source, parity * rows + way * quarter, quarter)
        sems = right_sem if way == 0 else left_sem
        return remote(ref, sent_ring_sem.at[way, step - 1], sems.at[step - 1], at_rank(along(sign)))

    def ring_arrival(step, way):
        sign = 1 if way == 0 else -1
        source = along(-sign * step)
        if step < half_way:
            ref = piece(source, parity * rows, rows)
        else:
            ref = piece(source, parity * rows + way * quarter, quarter)
        sems = right_sem if way == 0 else left_sem
        return remote(ref, sent_ring_sem.at[way, step - 1], sems.at[step - 1], at_rank(along(sign)))

    def cross(offset, way):
        source = along(offset)
        ref = piece(source, parity * rows + way * quarter, quarter)
        index = (offset + length) % length
        return remote(ref, sent_cross_sem.at[way, index], cross_sem.at[way, index], across(1 if way == 0 else -1))

    def cross_arrival(offset, way):
        source = along(offset)
        ref = piece(source, (1 - parity) * rows + way * quarter, quarter)
        index = (offset + length) % length
        return remote(ref, sent_cross_sem.at[way, index], cross_sem.at[way, index], across(1 if way == 0 else -1))

    def to_mate(offset, which):
        source = along(offset)
        index = (offset + length) % length
        start = (parity if which == 0 else 1 - parity) * rows
        return remote(piece(source, start, rows), sent_mate_sem.at[which, index], mate_sem.at[which, index], mate)

    def from_mate(offset, which):
        index = (offset + length) % length
        start = (parity if which == 0 else 1 - parity) * rows
        ref = weight_buf.at[along(offset) * 2 + 1 - core, pl.ds(pl.multiple_of(start, quarter), rows)]
        return remote(ref, sent_mate_sem.at[which, index], mate_sem.at[which, index], mate)

    def offsets(step):
        return [half_way] if step == half_way else [-step, step]

    for way in range(2):
        ring(1, way).start()
    for which in range(2):
        to_mate(0, which).start()

    def serve_ring(step):
        for way in range(2):
            ring_arrival(step, way).wait_recv()
            if step < half_way:
                ring(step + 1, way).start()
        for offset in offsets(step):
            for way in range(2):
                cross(offset, way).start()
            to_mate(offset, 0).start()

    served = set()

    def serve_cross(step):
        served.add(step)
        for offset in offsets(step):
            for way in range(2):
                cross_arrival(offset, way).wait_recv()
            to_mate(offset, 1).start()

    def head_copy(head, sender, target):
        return pltpu.make_async_remote_copy(
            src_ref=message_buf.at[head], dst_ref=arrive_buf.at[sender], send_sem=sent_sem, recv_sem=message_sem,
            device_id=target, device_id_type=MESH)

    def decay_copy(head, sender, target):
        return pltpu.make_async_remote_copy(
            src_ref=decay_buf.at[head], dst_ref=arrive_decay.at[sender], send_sem=sent_decay_sem,
            recv_sem=decay_sem, device_id=target, device_id_type=MESH)

    @pl.loop(0, pairs // batch)
    def _(b):
        ats = [pl.ds(pl.multiple_of((b * batch + i) * PAIR, PAIR), PAIR) for i in range(batch)]
        messages = transitions(size, ats, v_ref, ops, solved_bufs)
        for i, (first, second) in enumerate(messages):
            message_buf[2 * (b * batch + i)] = first
            message_buf[2 * (b * batch + i) + 1] = second
        count = 2 * batch

        @pl.loop(0, count)
        def _(j):
            head = b * count + lax.rem(me + j, count)

            @pl.when(head != my_head)
            def _():
                head_copy(head, me, {"sp": keeper(head)}).start()
                decay_copy(head, me, {"sp": keeper(head)}).start()

    arrive_buf[me] = message_buf[my_head]
    arrive_decay[me] = decay_buf[my_head]
    serve_ring(1)

    @pl.loop(0, pairs // batch)
    def _(b):
        for i in range(batch):
            readouts(size, pl.ds(pl.multiple_of((b * batch + i) * PAIR, PAIR), PAIR), v_ref, ops, solved_bufs,
                     local_bufs)

    serve_cross(1)
    if half_way > 1:
        serve_ring(2)

    others = pl.ds(0, devices - 1)
    pltpu.make_async_copy(arrive_buf.at[others], arrive_buf.at[others], message_sem).wait()
    pltpu.make_async_copy(arrive_decay.at[others], arrive_decay.at[others], decay_sem).wait()

    def back_copy(chunk, head, target):
        return pltpu.make_async_remote_copy(
            src_ref=back_buf.at[chunk], dst_ref=start_buf.at[head], send_sem=sent_back_sem, recv_sem=back_sem.at[head],
            device_id=target, device_id_type=MESH)

    row = iota((HEAD, PAIR), 0)
    lane = iota((HEAD, PAIR), 1)
    lower = lane < HEAD
    marker = jnp.where(lane == row + HEAD, F32(1.0), F32(0.0)).astype(BF16)
    marker = cat([jnp.zeros_like(marker), marker], 0)
    low_tall = iota((PAIR, PAIR), 1) < HEAD
    begin = jnp.where(iota((PAIR, PAIR), 0) == iota((PAIR, PAIR), 1), F32(1.0), F32(0.0))
    begin = jnp.where(low_tall, begin, 0.0)
    per = devices // XDIM
    steps = [[begin] for _ in range(XDIM)]
    for r in range(per):
        for g in range(XDIM):
            if g == XDIM - 1 and r == per - 1:
                continue
            c = g * per + r
            now = steps[g][-1]
            message = arrive_buf[c]
            moved = mm_nt(jnp.where(low_tall, now.astype(BF16), marker), cat([message, jnp.zeros_like(message)], 0))
            steps[g].append(moved + now * arrive_decay[c])

    def put_back(c, state):
        average = jnp.mean(state, axis=0, keepdims=True)
        centred = jnp.where(lower, state - average, 0.0)
        back_buf[c] = (centred[: HEAD // 2] + pltpu.roll(centred[HEAD // 2 :], HEAD, 1)).astype(BF16)

    state = jnp.zeros((HEAD, PAIR), F32)
    for g in range(XDIM):
        high, low = split(state)
        left = cat([jnp.where(lower, high, jnp.zeros_like(high)), jnp.where(lower, low, jnp.zeros_like(low))], 0)
        for r in range(per + 1):
            if g == XDIM - 1 and r == per:
                continue
            both = steps[g][r]
            if r == 0:
                reached = state
            elif g == 0:
                reached = both[HEAD:]
            else:
                moved = mm(left, both.astype(BF16))
                reached = moved[:HEAD] + moved[HEAD:] + both[HEAD:]
            if r < per:
                put_back(g * per + r, reached)
            else:
                state = reached

    @pl.loop(1, devices)
    def _(j):
        chunk = lax.rem(me + j, devices)
        back_copy(chunk, my_head, {"sp": chunk}).start()

    start_buf[my_head] = back_buf[me]

    if half_way > 1:
        serve_cross(2)
    for step in range(3, half_way + 1):
        serve_ring(step)
        if step < half_way:
            serve_cross(step)

    mean_ones = cat([same_head_ones(PAIR, 1.0 / HEAD)] * 2, 0)
    centring = jnp.where(lane == row + HEAD, F32(1.0 - 1.0 / HEAD), F32(-1.0 / HEAD)).astype(BF16)

    def finish_pair(p):
        at = pl.ds(pl.multiple_of(p * PAIR, PAIR), PAIR)
        wide = pl.ds(pl.multiple_of(p * QUAD, QUAD), QUAD)
        rights = []
        for i in range(2):
            head = 2 * p + i

            @pl.when(head != my_head)
            def _():
                back_copy(me, head, {"sp": me}).wait_recv()

            packed = start_buf[head]
            rights.append(jnp.where(lower, cat([packed, swap_halves(packed)], 0), centring))
        right = diag2(rights[0], rights[1])
        centred = mm_nt(local_high[:, wide], right) + mm_nt(local_low[:, wide], right)
        variance = mm(cat(split(centred * centred), 1), mean_ones)
        mix_buf[:, at] = (centred * lax.rsqrt(variance + 1.0) * gain_ref[:, at]).astype(BF16)

    @pl.loop(0, pairs // batch)
    def _(b):
        for i in range(batch):
            finish_pair(b * batch + i)

    def project(offset):
        at = along(offset)
        weight = cat([weight_buf[2 * at], weight_buf[2 * at + 1]], 1)
        out_ref[:, pl.ds(pl.multiple_of(at * QUAD, QUAD), QUAD)] = mm(mix_buf[...], weight).astype(BF16)

    for which in range(2):
        from_mate(0, which).wait_recv()
    project(0)
    for step in range(1, half_way + 1):
        if step not in served:
            serve_cross(step)
        for offset in offsets(step):
            for which in range(2):
                from_mate(offset, which).wait_recv()
        for offset in offsets(step):
            project(offset)

    pltpu.make_async_copy(message_buf.at[others], message_buf.at[others], sent_sem).wait()
    pltpu.make_async_copy(decay_buf.at[others], decay_buf.at[others], sent_decay_sem).wait()
    pltpu.make_async_copy(back_buf.at[others], back_buf.at[others], sent_back_sem).wait()
    for step in range(1, half_way + 1):
        for way in range(2):
            ring(step, way).wait_send()
        for offset in offsets(step):
            for way in range(2):
                cross(offset, way).wait_send()
            for which in range(2):
                to_mate(offset, which).wait_send()
    for which in range(2):
        to_mate(0, which).wait_send()


def per_device(devices, ranks, query_rows, key_rows, value_rows, decay_low, rate_low, decay_up, rate_up,
               decay_base, norm_gain, out_weight):
    size, width = query_rows.shape[1:]
    heads = width // HEAD
    batch = min(4, width // PAIR)
    length = ranks // 2
    half_way = length // 2
    vmem = pl.BlockSpec(memory_space=pltpu.VMEM)
    dma = pltpu.SemaphoreType.DMA
    wide = lambda lanes: pltpu.VMEM((size, lanes), BF16)
    out = pl.pallas_call(
        functools.partial(mixer_kernel, devices, ranks, batch),
        in_specs=[vmem] * 9 + [pl.BlockSpec(memory_space=pl.ANY)],
        out_specs=vmem,
        out_shape=jax.ShapeDtypeStruct((size, out_weight.shape[1] * ranks), BF16),
        scratch_shapes=[wide(width) for _ in range(10)] + [pltpu.VMEM((size, width), F32)] * 2
        + [wide(2 * width) for _ in range(4)] + [wide(width)] + [
            pltpu.VMEM((heads, HEAD, PAIR), BF16),
            pltpu.VMEM((heads, 1, PAIR), F32),
            pltpu.VMEM((devices, HEAD, PAIR), BF16),
            pltpu.VMEM((devices, 1, PAIR), F32),
            pltpu.VMEM((devices, HEAD // 2, PAIR), BF16),
            pltpu.VMEM((heads, HEAD // 2, PAIR), BF16),
            pltpu.VMEM((ranks,) + out_weight.shape, BF16),
            dma, dma, dma((heads,)), dma, dma, dma,
            dma((half_way,)), dma((half_way,)), dma((2, length)), dma((2, length)),
            dma((2, half_way)), dma((2, length)), dma((2, length)), dma,
        ],
        compiler_params=pltpu.CompilerParams(
            collective_id=0, has_side_effects=True, vmem_limit_bytes=60 * 2**20),
        cost_estimate=pl.CostEstimate(flops=10**10, bytes_accessed=10**7, transcendentals=0),
        name="mixer",
    )(query_rows[0], key_rows[0], value_rows[0], decay_low[0], rate_low[0], decay_up, rate_up,
      decay_base[None], norm_gain[None], out_weight)
    return out[None]


def solution(mesh):
    in_specs = (
        P("dp", "sp", None),
        P("dp", "sp", None),
        P("dp", "sp", None),
        P("dp", "sp", None),
        P("dp", "sp", None),
        P(),
        P(),
        P(),
        P(),
        P(None, "dp"),
    )
    return jax.shard_map(
        functools.partial(per_device, mesh.shape["sp"], mesh.shape["dp"]),
        mesh=mesh, in_specs=in_specs, out_specs=P("dp", "sp", None), check_vma=False,
    )
```

```python
import functools
import math

import jax
import jax.numpy as jnp
from jax import lax
from jax.experimental import pallas as pl
from jax.experimental.pallas import tpu as pltpu
from jax.sharding import PartitionSpec as P

HEAD = 64
PAIR = 2 * HEAD
QUAD = 2 * PAIR
XDIM = 4

F32 = jnp.float32
BF16 = jnp.bfloat16
MESH = pl.DeviceIdType.MESH


def mm(left, right):
    return lax.dot_general(left, right, (((1,), (0,)), ((), ())), preferred_element_type=F32)


def mm_nt(left, right):
    return lax.dot_general(left, right, (((1,), (1,)), ((), ())), preferred_element_type=F32)


def mm_tn(left, right):
    return lax.dot_general(left, right, (((0,), (0,)), ((), ())), preferred_element_type=F32)


def split(x):
    high = x.astype(BF16)
    return high, (x - high.astype(F32)).astype(BF16)


def iota(shape, dim):
    return lax.broadcasted_iota(jnp.int32, shape, dim)


def cat(parts, axis):
    return jnp.concatenate(parts, axis=axis)


def diag2(a, b):
    return cat([cat([a, jnp.zeros_like(b)], 1), cat([jnp.zeros_like(a), b], 1)], 0)


def swap_halves(x):
    return pltpu.roll(x.astype(F32), HEAD, 1).astype(x.dtype)


def low_half(shape):
    return lax.rem(iota(shape, 1), PAIR) < HEAD


def stack_pair(x):
    here = low_half(x.shape)
    zero = jnp.zeros_like(x)
    return cat([jnp.where(here, x, zero), jnp.where(here, zero, x)], 0)


def same_head_ones(width, scale):
    same = (iota((width, width), 0) // HEAD) == (iota((width, width), 1) // HEAD)
    return jnp.where(same, F32(scale), F32(0.0)).astype(BF16)


def put_split(refs, at, x):
    high, low = split(x)
    refs[0][:, at] = high
    refs[1][:, at] = low


def prepare(size, at, q_ref, k_ref, squashed, rate_low, dup_ref, rup_ref, base_ref, ops, decay_buf, pair):
    middle = size // 2
    upto = jnp.where(iota((size, size), 0) >= iota((size, size), 1), F32(1.0), F32(0.0)).astype(BF16)
    upto = cat([upto, upto], 1)
    decay_pre = (base_ref[:, at] + mm(squashed, dup_ref[:, at])).astype(BF16).astype(F32)
    rate_pre = mm(rate_low, rup_ref[:, at]).astype(BF16).astype(F32)
    log_decay = -math.exp(-0.5) / (1.0 + jnp.exp(-decay_pre))
    rate = 1.0 / (1.0 + jnp.exp(-rate_pre))
    running = mm(upto, cat(split(log_decay), 0))
    centre = running[middle : middle + 1]
    final = running[size - 1 :]
    ahead = jnp.exp(running - centre)
    before = jnp.exp(running - log_decay - centre)
    behind = jnp.exp(centre - running)
    at_centre = jnp.exp(centre)
    at_end = jnp.exp(final - centre)
    k = k_ref[:, at].astype(F32)
    q = q_ref[:, at].astype(F32)
    unit = k * lax.rsqrt(1.0 + mm(cat(split(k * k), 1), cat([same_head_ones(QUAD, 1.0)] * 2, 0)))
    erase_from = unit * before
    read_mid = q * ahead
    key_to = k * behind
    erase_to = -(unit * rate) * behind
    put_split(ops["from"], at, erase_from)
    put_split(ops["read"], at, read_mid)
    put_split(ops["key"], at, key_to)
    put_split(ops["erase"], at, erase_to)
    ops["from_start"][:, at] = erase_from * at_centre
    ops["read_start"][:, at] = read_mid * at_centre
    ops["key_end"][:, at] = (key_to * at_end).astype(BF16)
    ops["erase_end"][:, at] = (erase_to * at_end).astype(BF16)
    decays = jnp.exp(final)
    for i in range(2):
        here = decays[:, i * PAIR : (i + 1) * PAIR]
        decay_buf[2 * (pair + i)] = here
        decay_buf[2 * (pair + i) + 1] = pltpu.roll(here, HEAD, 1)


def by_head(x):
    return diag2(x[:, :PAIR], x[:, PAIR:])


def grids(size, left, ops, at, keep):
    high, low = (stack_pair(ref[:, at]) for ref in left)
    right = cat([ops["key"][0][:, at], ops["erase"][0][:, at]], 0)
    rest = cat([ops["key"][1][:, at], ops["erase"][1][:, at]], 0)
    grid = mm_nt(cat([high, low], 1), cat([right, right], 1)) + mm_nt(high, rest)
    part = lambda i, j: jnp.where(keep, grid[i * size : (i + 1) * size, j * size : (j + 1) * size], 0.0)
    return split(cat([part(0, 0), part(1, 0)], 1)), split(cat([part(0, 1), part(1, 1)], 1))


def inverses(splits, size):
    negs = [high for high, _ in splits]
    row = iota((size, PAIR * 2), 0)
    col = lax.rem(iota((size, PAIR * 2), 1), PAIR)
    eye = jnp.where(row == col, F32(1.0), F32(0.0)).astype(BF16)
    found = None
    block = 1
    while block < size:
        pick = (row // (2 * block) == col // (2 * block)) & (row // block != col // block) & (row > col)
        pieces = [jnp.where(pick, n, jnp.zeros_like(n)) for n in negs]
        if found is None:
            found = [eye + p for p in pieces]
        elif block < 16:
            right = [mm(p, by_head(x)).astype(BF16) for p, x in zip(pieces, found)]
            found = [x + mm(x, by_head(y)).astype(BF16) for x, y in zip(found, right)]
        else:
            starts = list(range(block, size, 2 * block))
            take = lambda m: cat([m[s : s + block] for s in starts], 0) if len(starts) > 1 else m[block:]
            right = [mm(take(p), by_head(x)).astype(BF16) for p, x in zip(pieces, found)]
            blank = jnp.zeros((block, 2 * PAIR), BF16)
            spread = lambda m: cat(
                [part for j in range(len(starts)) for part in (blank, m[j * block : (j + 1) * block])], 0)
            right = [spread(y) for y in right]
            step = [mm(take(x), by_head(y)).astype(BF16) for x, y in zip(found, right)]
            found = [x + spread(t) for x, t in zip(found, step)]
        block *= 2
    out = []
    for (high, low), x in zip(splits, found):
        residual = (eye - x).astype(F32) + (mm(high, by_head(x)) + mm(low, by_head(x)))
        out.append((x, mm(x, by_head(residual.astype(BF16))).astype(BF16)))
    return out


def low_part(x):
    return jnp.where(low_half(x.shape), x, jnp.zeros_like(x))


def high_part(x):
    return jnp.where(low_half(x.shape), jnp.zeros_like(x), x)


def transitions(size, ats, v_ref, ops, solved_bufs):
    strict = iota((size, size), 0) > iota((size, size), 1)
    negs, sides = [], []
    for at in ats:
        keys, neg = grids(size, ops["from"], ops, at, strict)
        negs.append(neg)
        v = v_ref[:, at]
        values = diag2(high_part(swap_halves(v)), high_part(v))
        carried = mm(keys[0], values) + mm(keys[1], values)
        base = ops["from_start"][:, at]
        lows = cat([low_part(base), low_part(swap_halves(base))], 1)
        sides.append(split(lows + carried))
    found = inverses(negs, size)
    messages = []
    for at, x, side in zip(ats, found, sides):
        solved = split(mm(x[0], by_head(side[0])) + mm(x[0], by_head(side[1])) + mm(x[1], by_head(side[0])))
        wide = pl.ds(pl.multiple_of(2 * at.start, QUAD), QUAD)
        solved_bufs[0][:, wide] = solved[0]
        solved_bufs[1][:, wide] = solved[1]
        v = v_ref[:, at]
        ends = cat([ops["erase_end"][:, at], ops["key_end"][:, at]], 0)
        values = cat([high_part(swap_halves(v)), high_part(v)], 1)
        made = mm_tn(ends, cat([solved[0], values], 0)).astype(BF16)
        messages.append((made[:HEAD, :PAIR], made[HEAD:, PAIR:]))
    return messages


def readouts(size, at, v_ref, ops, solved_bufs, local_bufs):
    within = iota((size, size), 0) >= iota((size, size), 1)
    keys, erases = grids(size, ops["read"], ops, at, within)
    left = [cat([e[:, :PAIR], k[:, :PAIR], e[:, PAIR:], k[:, PAIR:]], 1) for k, e in zip(keys, erases)]
    wide = pl.ds(pl.multiple_of(2 * at.start, QUAD), QUAD)
    solved = solved_bufs[0][:, wide]
    v = v_ref[:, at]
    right = diag2(cat([solved[:, :PAIR], high_part(swap_halves(v))], 0), cat([solved[:, PAIR:], high_part(v)], 0))
    base = ops["read_start"][:, at]
    lows = cat([low_part(base), low_part(swap_halves(base))], 1)
    taken = mm(left[0], right) + mm(left[1], right) + mm(erases[0], by_head(solved_bufs[1][:, wide]))
    put_split(local_bufs, wide, lows + taken)


def mixer_kernel(devices, ranks, batch,
                 q_ref, k_ref, v_ref, low_ref, rate_ref, dup_ref, rup_ref, base_ref, gain_ref, w_ref,
                 out_ref,
                 from_high, from_low, read_high, read_low, key_high, key_low, erase_high, erase_low,
                 key_end, erase_end, from_start, read_start,
                 solved_high, solved_low, local_high, local_low, mix_buf,
                 message_buf, decay_buf, arrive_buf, arrive_decay, back_buf, start_buf, weight_buf,
                 message_sem, decay_sem, back_sem, sent_sem, sent_decay_sem, sent_back_sem,
                 right_sem, left_sem, cross_sem, mate_sem, sent_ring_sem, sent_cross_sem, sent_mate_sem, own_sem):
    size, width = q_ref.shape
    pairs = width // PAIR
    ops = {"from": (from_high, from_low), "read": (read_high, read_low), "key": (key_high, key_low),
           "erase": (erase_high, erase_low), "key_end": key_end, "erase_end": erase_end,
           "from_start": from_start, "read_start": read_start}
    solved_bufs = (solved_high, solved_low)
    local_bufs = (local_high, local_low)
    me = lax.axis_index("sp")
    rank = lax.axis_index("dp")
    length = ranks // 2
    half_way = length // 2
    core = lax.rem(rank, 2)
    line = rank // 2
    along = lambda step: lax.rem(line + step + length, length)
    at_rank = lambda row: {"dp": row * 2 + core}
    mate = {"dp": rank + 1 - 2 * core}
    x = lax.rem(me, XDIM)
    across = lambda step: {"sp": me - x + lax.rem(x + step + XDIM, XDIM)}
    parity = lax.rem(x, 2)
    rows = width // 2
    quarter = rows // 2

    planes = devices // XDIM
    plane = me // XDIM
    my_head = lax.rem(x + planes * XDIM - plane, XDIM) * planes + plane

    def keeper(head):
        place = lax.rem(head, planes)
        return place * XDIM + lax.rem(place + head // planes, XDIM)

    barrier = pltpu.get_barrier_semaphore()

    @pl.loop(1, devices)
    def _(j):
        pl.semaphore_signal(barrier, inc=1, device_id={"sp": lax.rem(me + j, devices)}, device_id_type=MESH)

    for target in (at_rank(along(1)), at_rank(along(-1)), mate):
        pl.semaphore_signal(barrier, inc=1, device_id=target, device_id_type=MESH)
    own = pltpu.make_async_copy(w_ref, weight_buf.at[rank], own_sem)
    own.start()

    squashed = jnp.tanh(low_ref[...].astype(F32)).astype(BF16)
    rate_low = rate_ref[...]

    def prepare_quads(quads):
        for i in quads:
            prepare(size, pl.ds(pl.multiple_of(i * QUAD, QUAD), QUAD), q_ref, k_ref, squashed, rate_low,
                    dup_ref, rup_ref, base_ref, ops, decay_buf, i * 2)

    piece = lambda source, start, count: weight_buf.at[
        source * 2 + core, pl.ds(pl.multiple_of(start, quarter), count)]

    def remote(ref, sem_out, sem_in, target):
        return pltpu.make_async_remote_copy(
            src_ref=ref, dst_ref=ref, send_sem=sem_out, recv_sem=sem_in, device_id=target, device_id_type=MESH)

    def ring(step, way):
        sign = 1 if way == 0 else -1
        source = along(-sign * (step - 1))
        if step < half_way:
            ref = piece(source, parity * rows, rows)
        else:
            ref = piece(source, parity * rows + way * quarter, quarter)
        sems = right_sem if way == 0 else left_sem
        return remote(ref, sent_ring_sem.at[way, step - 1], sems.at[step - 1], at_rank(along(sign)))

    def ring_arrival(step, way):
        sign = 1 if way == 0 else -1
        source = along(-sign * step)
        if step < half_way:
            ref = piece(source, parity * rows, rows)
        else:
            ref = piece(source, parity * rows + way * quarter, quarter)
        sems = right_sem if way == 0 else left_sem
        return remote(ref, sent_ring_sem.at[way, step - 1], sems.at[step - 1], at_rank(along(sign)))

    def cross(offset, way):
        source = along(offset)
        ref = piece(source, parity * rows + way * quarter, quarter)
        index = (offset + length) % length
        return remote(ref, sent_cross_sem.at[way, index], cross_sem.at[way, index], across(1 if way == 0 else -1))

    def cross_arrival(offset, way):
        source = along(offset)
        ref = piece(source, (1 - parity) * rows + way * quarter, quarter)
        index = (offset + length) % length
        return remote(ref, sent_cross_sem.at[way, index], cross_sem.at[way, index], across(1 if way == 0 else -1))

    def to_mate(offset, which):
        source = along(offset)
        index = (offset + length) % length
        start = (parity if which == 0 else 1 - parity) * rows
        return remote(piece(source, start, rows), sent_mate_sem.at[which, index], mate_sem.at[which, index], mate)

    def from_mate(offset, which):
        index = (offset + length) % length
        start = (parity if which == 0 else 1 - parity) * rows
        ref = weight_buf.at[along(offset) * 2 + 1 - core, pl.ds(pl.multiple_of(start, quarter), rows)]
        return remote(ref, sent_mate_sem.at[which, index], mate_sem.at[which, index], mate)

    def offsets(step):
        return [half_way] if step == half_way else [-step, step]

    def serve_ring(step):
        for way in range(2):
            ring_arrival(step, way).wait_recv()
            if step < half_way:
                ring(step + 1, way).start()
        for offset in offsets(step):
            for way in range(2):
                cross(offset, way).start()
            to_mate(offset, 0).start()

    served = set()

    def serve_cross(step):
        served.add(step)
        for offset in offsets(step):
            for way in range(2):
                cross_arrival(offset, way).wait_recv()
            to_mate(offset, 1).start()

    @pl.loop(0, pairs // batch)
    def _(b):
        prepare_quads([b * (batch // 2) + i for i in range(batch // 2)])

        @pl.when(b == 0)
        def _():
            pl.semaphore_wait(barrier, devices - 1 + 3)
            own.wait()
            for way in range(2):
                ring(1, way).start()
            for which in range(2):
                to_mate(0, which).start()

    def head_copy(head, sender, target):
        return pltpu.make_async_remote_copy(
            src_ref=message_buf.at[head], dst_ref=arrive_buf.at[sender], send_sem=sent_sem, recv_sem=message_sem,
            device_id=target, device_id_type=MESH)

    def decay_copy(head, sender, target):
        return pltpu.make_async_remote_copy(
            src_ref=decay_buf.at[head], dst_ref=arrive_decay.at[sender], send_sem=sent_decay_sem,
            recv_sem=decay_sem, device_id=target, device_id_type=MESH)

    @pl.loop(0, pairs // batch)
    def _(b):
        ats = [pl.ds(pl.multiple_of((b * batch + i) * PAIR, PAIR), PAIR) for i in range(batch)]
        messages = transitions(size, ats, v_ref, ops, solved_bufs)
        for i, (first, second) in enumerate(messages):
            message_buf[2 * (b * batch + i)] = first
            message_buf[2 * (b * batch + i) + 1] = second
        count = 2 * batch

        @pl.loop(0, count)
        def _(j):
            head = b * count + lax.rem(me + j, count)

            @pl.when(head != my_head)
            def _():
                head_copy(head, me, {"sp": keeper(head)}).start()
                decay_copy(head, me, {"sp": keeper(head)}).start()

        @pl.when(b == 0)
        def _():
            serve_ring(1)

    arrive_buf[me] = message_buf[my_head]
    arrive_decay[me] = decay_buf[my_head]
    serve_cross(1)
    if half_way > 1:
        serve_ring(2)

    @pl.loop(0, pairs // batch)
    def _(b):
        for i in range(batch):
            readouts(size, pl.ds(pl.multiple_of((b * batch + i) * PAIR, PAIR), PAIR), v_ref, ops, solved_bufs,
                     local_bufs)

    if half_way > 1:
        serve_cross(2)
    if half_way > 2:
        serve_ring(3)

    others = pl.ds(0, devices - 1)
    pltpu.make_async_copy(arrive_buf.at[others], arrive_buf.at[others], message_sem).wait()
    pltpu.make_async_copy(arrive_decay.at[others], arrive_decay.at[others], decay_sem).wait()

    def back_copy(chunk, head, target):
        return pltpu.make_async_remote_copy(
            src_ref=back_buf.at[chunk], dst_ref=start_buf.at[head], send_sem=sent_back_sem, recv_sem=back_sem.at[head],
            device_id=target, device_id_type=MESH)

    row = iota((HEAD, PAIR), 0)
    lane = iota((HEAD, PAIR), 1)
    lower = lane < HEAD
    marker = jnp.where(lane == row + HEAD, F32(1.0), F32(0.0)).astype(BF16)
    marker = cat([jnp.zeros_like(marker), marker], 0)
    low_tall = iota((PAIR, PAIR), 1) < HEAD
    begin = jnp.where(iota((PAIR, PAIR), 0) == iota((PAIR, PAIR), 1), F32(1.0), F32(0.0))
    begin = jnp.where(low_tall, begin, 0.0)
    per = devices // XDIM
    steps = [[begin] for _ in range(XDIM)]
    for r in range(per):
        for g in range(XDIM):
            if g == XDIM - 1 and r == per - 1:
                continue
            c = g * per + r
            now = steps[g][-1]
            message = arrive_buf[c]
            moved = mm_nt(jnp.where(low_tall, now.astype(BF16), marker), cat([message, jnp.zeros_like(message)], 0))
            steps[g].append(moved + now * arrive_decay[c])

    def put_back(c, state):
        average = jnp.mean(state, axis=0, keepdims=True)
        centred = jnp.where(lower, state - average, 0.0)
        back_buf[c] = (centred[: HEAD // 2] + pltpu.roll(centred[HEAD // 2 :], HEAD, 1)).astype(BF16)

    state = jnp.zeros((HEAD, PAIR), F32)
    for g in range(XDIM):
        high, low = split(state)
        left = cat([jnp.where(lower, high, jnp.zeros_like(high)), jnp.where(lower, low, jnp.zeros_like(low))], 0)
        for r in range(per + 1):
            if g == XDIM - 1 and r == per:
                continue
            both = steps[g][r]
            if r == 0:
                reached = state
            elif g == 0:
                reached = both[HEAD:]
            else:
                moved = mm(left, both.astype(BF16))
                reached = moved[:HEAD] + moved[HEAD:] + both[HEAD:]
            if r < per:
                put_back(g * per + r, reached)
            else:
                state = reached

    @pl.loop(1, devices)
    def _(j):
        chunk = lax.rem(me + j, devices)
        back_copy(chunk, my_head, {"sp": chunk}).start()

    start_buf[my_head] = back_buf[me]

    for step in range(3, half_way):
        serve_cross(step)
        serve_ring(step + 1)

    mean_ones = cat([same_head_ones(PAIR, 1.0 / HEAD)] * 2, 0)
    centring = jnp.where(lane == row + HEAD, F32(1.0 - 1.0 / HEAD), F32(-1.0 / HEAD)).astype(BF16)

    def finish_wait(p):
        for i in range(2):
            head = 2 * p + i

            @pl.when(head != my_head)
            def _():
                back_copy(me, head, {"sp": me}).wait_recv()

    def finish_pair(p):
        at = pl.ds(pl.multiple_of(p * PAIR, PAIR), PAIR)
        wide = pl.ds(pl.multiple_of(p * QUAD, QUAD), QUAD)
        rights = []
        for i in range(2):
            packed = start_buf[2 * p + i]
            rights.append(jnp.where(lower, cat([packed, swap_halves(packed)], 0), centring))
        right = diag2(rights[0], rights[1])
        centred = mm_nt(local_high[:, wide], right) + mm_nt(local_low[:, wide], right)
        variance = mm(cat(split(centred * centred), 1), mean_ones)
        mix_buf[:, at] = (centred * lax.rsqrt(variance + 1.0) * gain_ref[:, at]).astype(BF16)

    @pl.loop(0, pairs // batch)
    def _(b):
        for i in range(batch):
            finish_wait(b * batch + i)
        for i in range(batch):
            finish_pair(b * batch + i)

    def project(offset):
        at = along(offset)
        weight = cat([weight_buf[2 * at], weight_buf[2 * at + 1]], 1)
        out_ref[:, pl.ds(pl.multiple_of(at * QUAD, QUAD), QUAD)] = mm(mix_buf[...], weight).astype(BF16)

    last = [step for step in range(1, half_way + 1) if step not in served]
    early = [offset for step in range(1, half_way) for offset in offsets(step)]
    for offset in [0] + early:
        for which in range(2):
            from_mate(offset, which).wait_recv()
    for step in last:
        serve_cross(step)
    for offset in [0] + early:
        project(offset)
    for which in range(2):
        from_mate(half_way, which).wait_recv()
    project(half_way)

    pltpu.make_async_copy(message_buf.at[others], message_buf.at[others], sent_sem).wait()
    pltpu.make_async_copy(decay_buf.at[others], decay_buf.at[others], sent_decay_sem).wait()
    pltpu.make_async_copy(back_buf.at[others], back_buf.at[others], sent_back_sem).wait()
    for step in range(1, half_way + 1):
        for way in range(2):
            ring(step, way).wait_send()
        for offset in offsets(step):
            for way in range(2):
                cross(offset, way).wait_send()
            for which in range(2):
                to_mate(offset, which).wait_send()
    for which in range(2):
        to_mate(0, which).wait_send()


def per_device(devices, ranks, query_rows, key_rows, value_rows, decay_low, rate_low, decay_up, rate_up,
               decay_base, norm_gain, out_weight):
    size, width = query_rows.shape[1:]
    heads = width // HEAD
    batch = min(8, width // PAIR)
    length = ranks // 2
    half_way = length // 2
    vmem = pl.BlockSpec(memory_space=pltpu.VMEM)
    dma = pltpu.SemaphoreType.DMA
    wide = lambda lanes: pltpu.VMEM((size, lanes), BF16)
    out = pl.pallas_call(
        functools.partial(mixer_kernel, devices, ranks, batch),
        in_specs=[vmem] * 9 + [pl.BlockSpec(memory_space=pl.ANY)],
        out_specs=vmem,
        out_shape=jax.ShapeDtypeStruct((size, out_weight.shape[1] * ranks), BF16),
        scratch_shapes=[wide(width) for _ in range(10)] + [pltpu.VMEM((size, width), F32)] * 2
        + [wide(2 * width) for _ in range(4)] + [wide(width)] + [
            pltpu.VMEM((heads, HEAD, PAIR), BF16),
            pltpu.VMEM((heads, 1, PAIR), F32),
            pltpu.VMEM((devices, HEAD, PAIR), BF16),
            pltpu.VMEM((devices, 1, PAIR), F32),
            pltpu.VMEM((devices, HEAD // 2, PAIR), BF16),
            pltpu.VMEM((heads, HEAD // 2, PAIR), BF16),
            pltpu.VMEM((ranks,) + out_weight.shape, BF16),
            dma, dma, dma((heads,)), dma, dma, dma,
            dma((half_way,)), dma((half_way,)), dma((2, length)), dma((2, length)),
            dma((2, half_way)), dma((2, length)), dma((2, length)), dma,
        ],
        compiler_params=pltpu.CompilerParams(
            collective_id=0, has_side_effects=True, vmem_limit_bytes=60 * 2**20),
        cost_estimate=pl.CostEstimate(flops=10**10, bytes_accessed=10**7, transcendentals=0),
        name="mixer",
    )(query_rows[0], key_rows[0], value_rows[0], decay_low[0], rate_low[0], decay_up, rate_up,
      decay_base[None], norm_gain[None], out_weight)
    return out[None]


def solution(mesh):
    in_specs = (
        P("dp", "sp", None),
        P("dp", "sp", None),
        P("dp", "sp", None),
        P("dp", "sp", None),
        P("dp", "sp", None),
        P(),
        P(),
        P(),
        P(),
        P(None, "dp"),
    )
    return jax.shard_map(
        functools.partial(per_device, mesh.shape["sp"], mesh.shape["dp"]),
        mesh=mesh, in_specs=in_specs, out_specs=P("dp", "sp", None), check_vma=False,
    )
```

```python
import functools
import math

import jax
import jax.numpy as jnp
from jax import lax
from jax.experimental import pallas as pl
from jax.experimental.pallas import tpu as pltpu
from jax.sharding import PartitionSpec as P

HEAD = 64
PAIR = 2 * HEAD
QUAD = 2 * PAIR
XDIM = 4

F32 = jnp.float32
BF16 = jnp.bfloat16
MESH = pl.DeviceIdType.MESH


def mm(left, right):
    return lax.dot_general(left, right, (((1,), (0,)), ((), ())), preferred_element_type=F32)


def mm_nt(left, right):
    return lax.dot_general(left, right, (((1,), (1,)), ((), ())), preferred_element_type=F32)


def mm_tn(left, right):
    return lax.dot_general(left, right, (((0,), (0,)), ((), ())), preferred_element_type=F32)


def split(x):
    high = x.astype(BF16)
    return high, (x - high.astype(F32)).astype(BF16)


def iota(shape, dim):
    return lax.broadcasted_iota(jnp.int32, shape, dim)


def cat(parts, axis):
    return jnp.concatenate(parts, axis=axis)


def diag2(a, b):
    return cat([cat([a, jnp.zeros_like(b)], 1), cat([jnp.zeros_like(a), b], 1)], 0)


def swap_halves(x):
    return pltpu.roll(x.astype(F32), HEAD, 1).astype(x.dtype)


def low_half(shape):
    return lax.rem(iota(shape, 1), PAIR) < HEAD


def stack_pair(x):
    here = low_half(x.shape)
    zero = jnp.zeros_like(x)
    return cat([jnp.where(here, x, zero), jnp.where(here, zero, x)], 0)


def same_head_ones(width, scale):
    same = (iota((width, width), 0) // HEAD) == (iota((width, width), 1) // HEAD)
    return jnp.where(same, F32(scale), F32(0.0)).astype(BF16)


def put_split(refs, at, x):
    high, low = split(x)
    refs[0][:, at] = high
    refs[1][:, at] = low


def wavefront(works):
    running = []
    waiting = list(works)
    while waiting or running:
        if waiting:
            running.append(waiting.pop(0))
        running = [work for work in running if next(work, 0) is None]


def prepare(size, at, q_ref, k_ref, squashed, rate_low, dup_ref, rup_ref, base_ref, ops, decay_buf, pair):
    middle = size // 2
    upto = jnp.where(iota((size, size), 0) >= iota((size, size), 1), F32(1.0), F32(0.0)).astype(BF16)
    upto = cat([upto, upto], 1)
    decay_pre = mm(squashed, dup_ref[:, at])
    rate_pre = mm(rate_low, rup_ref[:, at])
    yield
    decay_pre = (base_ref[:, at] + decay_pre).astype(BF16).astype(F32)
    rate_pre = rate_pre.astype(BF16).astype(F32)
    log_decay = -math.exp(-0.5) / (1.0 + jnp.exp(-decay_pre))
    rate = 1.0 / (1.0 + jnp.exp(-rate_pre))
    running = mm(upto, cat(split(log_decay), 0))
    k = k_ref[:, at].astype(F32)
    norm = mm(cat(split(k * k), 1), cat([same_head_ones(QUAD, 1.0)] * 2, 0))
    yield
    centre = running[middle : middle + 1]
    final = running[size - 1 :]
    shifted = running - centre
    ahead = jnp.exp(shifted)
    before = jnp.exp(shifted - log_decay)
    behind = jnp.exp(-shifted)
    at_centre = jnp.exp(centre)
    at_end = jnp.exp(final - centre)
    q = q_ref[:, at].astype(F32)
    unit = k * lax.rsqrt(1.0 + norm)
    erase_from = unit * before
    read_mid = q * ahead
    key_to = k * behind
    erase_to = -(unit * rate) * behind
    put_split(ops["from"], at, erase_from)
    put_split(ops["read"], at, read_mid)
    put_split(ops["key"], at, key_to)
    put_split(ops["erase"], at, erase_to)
    ops["from_start"][:, at] = erase_from * at_centre
    ops["read_start"][:, at] = read_mid * at_centre
    ops["key_end"][:, at] = (key_to * at_end).astype(BF16)
    ops["erase_end"][:, at] = (erase_to * at_end).astype(BF16)
    decays = jnp.exp(final)
    for i in range(2):
        here = decays[:, i * PAIR : (i + 1) * PAIR]
        decay_buf[2 * (pair + i)] = here
        decay_buf[2 * (pair + i) + 1] = pltpu.roll(here, HEAD, 1)


def by_head(x):
    return diag2(x[:, :PAIR], x[:, PAIR:])


def raw_grid(left, ops, at):
    high, low = (stack_pair(ref[:, at]) for ref in left)
    right = cat([ops["key"][0][:, at], ops["erase"][0][:, at]], 0)
    rest = cat([ops["key"][1][:, at], ops["erase"][1][:, at]], 0)
    return mm_nt(cat([high, low], 1), cat([right, right], 1)) + mm_nt(high, rest)


def grid_parts(size, grid, keep):
    part = lambda i, j: jnp.where(keep, grid[i * size : (i + 1) * size, j * size : (j + 1) * size], 0.0)
    return split(cat([part(0, 0), part(1, 0)], 1)), split(cat([part(0, 1), part(1, 1)], 1))


def inverses(splits, size):
    negs = [high for high, _ in splits]
    row = iota((size, PAIR * 2), 0)
    col = lax.rem(iota((size, PAIR * 2), 1), PAIR)
    eye = jnp.where(row == col, F32(1.0), F32(0.0)).astype(BF16)
    found = None
    block = 1
    while block < size:
        pick = (row // (2 * block) == col // (2 * block)) & (row // block != col // block) & (row > col)
        pieces = [jnp.where(pick, n, jnp.zeros_like(n)) for n in negs]
        if found is None:
            found = [eye + p for p in pieces]
        elif block < 16:
            right = [mm(p, by_head(x)).astype(BF16) for p, x in zip(pieces, found)]
            found = [x + mm(x, by_head(y)).astype(BF16) for x, y in zip(found, right)]
        else:
            starts = list(range(block, size, 2 * block))
            take = lambda m: cat([m[s : s + block] for s in starts], 0) if len(starts) > 1 else m[block:]
            right = [mm(take(p), by_head(x)).astype(BF16) for p, x in zip(pieces, found)]
            blank = jnp.zeros((block, 2 * PAIR), BF16)
            spread = lambda m: cat(
                [part for j in range(len(starts)) for part in (blank, m[j * block : (j + 1) * block])], 0)
            right = [spread(y) for y in right]
            step = [mm(take(x), by_head(y)).astype(BF16) for x, y in zip(found, right)]
            found = [x + spread(t) for x, t in zip(found, step)]
        block *= 2
    left = [mm(high, by_head(x)) + mm(low, by_head(x)) for (high, low), x in zip(splits, found)]
    left = [((eye - x).astype(F32) + r).astype(BF16) for x, r in zip(found, left)]
    return [(x, mm(x, by_head(r)).astype(BF16)) for x, r in zip(found, left)]


def low_part(x):
    return jnp.where(low_half(x.shape), x, jnp.zeros_like(x))


def high_part(x):
    return jnp.where(low_half(x.shape), jnp.zeros_like(x), x)


def transitions(size, ats, v_ref, ops, solved_bufs):
    strict = iota((size, size), 0) > iota((size, size), 1)
    negs, sides = [], []

    def front(at):
        grid = raw_grid(ops["from"], ops, at)
        yield
        keys, neg = grid_parts(size, grid, strict)
        negs.append(neg)
        v = v_ref[:, at]
        values = diag2(high_part(swap_halves(v)), high_part(v))
        carried = mm(keys[0], values) + mm(keys[1], values)
        yield
        base = ops["from_start"][:, at]
        lows = cat([low_part(base), low_part(swap_halves(base))], 1)
        sides.append(split(lows + carried))

    wavefront([front(at) for at in ats])
    found = inverses(negs, size)
    solved = [split(mm(x[0], by_head(side[0])) + mm(x[0], by_head(side[1])) + mm(x[1], by_head(side[0])))
              for x, side in zip(found, sides)]
    made = []
    for at, parts in zip(ats, solved):
        wide = pl.ds(pl.multiple_of(2 * at.start, QUAD), QUAD)
        solved_bufs[0][:, wide] = parts[0]
        solved_bufs[1][:, wide] = parts[1]
        v = v_ref[:, at]
        ends = cat([ops["erase_end"][:, at], ops["key_end"][:, at]], 0)
        values = cat([high_part(swap_halves(v)), high_part(v)], 1)
        made.append(mm_tn(ends, cat([parts[0], values], 0)))
    return [(m[:HEAD, :PAIR].astype(BF16), m[HEAD:, PAIR:].astype(BF16)) for m in made]


def readouts(size, at, v_ref, ops, solved_bufs, local_bufs):
    within = iota((size, size), 0) >= iota((size, size), 1)
    grid = raw_grid(ops["read"], ops, at)
    yield
    keys, erases = grid_parts(size, grid, within)
    left = [cat([e[:, :PAIR], k[:, :PAIR], e[:, PAIR:], k[:, PAIR:]], 1) for k, e in zip(keys, erases)]
    wide = pl.ds(pl.multiple_of(2 * at.start, QUAD), QUAD)
    solved = solved_bufs[0][:, wide]
    v = v_ref[:, at]
    right = diag2(cat([solved[:, :PAIR], high_part(swap_halves(v))], 0), cat([solved[:, PAIR:], high_part(v)], 0))
    taken = mm(left[0], right) + mm(left[1], right) + mm(erases[0], by_head(solved_bufs[1][:, wide]))
    yield
    base = ops["read_start"][:, at]
    lows = cat([low_part(base), low_part(swap_halves(base))], 1)
    put_split(local_bufs, wide, lows + taken)


def mixer_kernel(devices, ranks, batch,
                 q_ref, k_ref, v_ref, low_ref, rate_ref, dup_ref, rup_ref, base_ref, gain_ref, w_ref,
                 out_ref,
                 from_high, from_low, read_high, read_low, key_high, key_low, erase_high, erase_low,
                 key_end, erase_end, from_start, read_start,
                 solved_high, solved_low, local_high, local_low, mix_buf,
                 message_buf, decay_buf, arrive_buf, arrive_decay, back_buf, start_buf, weight_buf,
                 message_sem, decay_sem, back_sem, sent_sem, sent_decay_sem, sent_back_sem,
                 right_sem, left_sem, cross_sem, mate_sem, sent_ring_sem, sent_cross_sem, sent_mate_sem, own_sem):
    size, width = q_ref.shape
    pairs = width // PAIR
    ops = {"from": (from_high, from_low), "read": (read_high, read_low), "key": (key_high, key_low),
           "erase": (erase_high, erase_low), "key_end": key_end, "erase_end": erase_end,
           "from_start": from_start, "read_start": read_start}
    solved_bufs = (solved_high, solved_low)
    local_bufs = (local_high, local_low)
    me = lax.axis_index("sp")
    rank = lax.axis_index("dp")
    length = ranks // 2
    half_way = length // 2
    core = lax.rem(rank, 2)
    line = rank // 2
    along = lambda step: lax.rem(line + step + length, length)
    at_rank = lambda row: {"dp": row * 2 + core}
    mate = {"dp": rank + 1 - 2 * core}
    x = lax.rem(me, XDIM)
    across = lambda step: {"sp": me - x + lax.rem(x + step + XDIM, XDIM)}
    parity = lax.rem(x, 2)
    rows = width // 2
    quarter = rows // 2

    planes = devices // XDIM
    plane = me // XDIM
    my_head = lax.rem(x + planes * XDIM - plane, XDIM) * planes + plane

    def keeper(head):
        place = lax.rem(head, planes)
        return place * XDIM + lax.rem(place + head // planes, XDIM)

    barrier = pltpu.get_barrier_semaphore()

    @pl.loop(1, devices)
    def _(j):
        pl.semaphore_signal(barrier, inc=1, device_id={"sp": lax.rem(me + j, devices)}, device_id_type=MESH)

    for target in (at_rank(along(1)), at_rank(along(-1)), mate):
        pl.semaphore_signal(barrier, inc=1, device_id=target, device_id_type=MESH)
    own = pltpu.make_async_copy(w_ref, weight_buf.at[rank], own_sem)
    own.start()

    squashed = jnp.tanh(low_ref[...].astype(F32)).astype(BF16)
    rate_low = rate_ref[...]

    def prepare_quads(quads):
        wavefront([prepare(size, pl.ds(pl.multiple_of(i * QUAD, QUAD), QUAD), q_ref, k_ref, squashed, rate_low,
                           dup_ref, rup_ref, base_ref, ops, decay_buf, i * 2) for i in quads])

    piece = lambda source, start, count: weight_buf.at[
        source * 2 + core, pl.ds(pl.multiple_of(start, quarter), count)]

    def remote(ref, sem_out, sem_in, target):
        return pltpu.make_async_remote_copy(
            src_ref=ref, dst_ref=ref, send_sem=sem_out, recv_sem=sem_in, device_id=target, device_id_type=MESH)

    def ring(step, way):
        sign = 1 if way == 0 else -1
        source = along(-sign * (step - 1))
        if step < half_way:
            ref = piece(source, parity * rows, rows)
        else:
            ref = piece(source, parity * rows + way * quarter, quarter)
        sems = right_sem if way == 0 else left_sem
        return remote(ref, sent_ring_sem.at[way, step - 1], sems.at[step - 1], at_rank(along(sign)))

    def ring_arrival(step, way):
        sign = 1 if way == 0 else -1
        source = along(-sign * step)
        if step < half_way:
            ref = piece(source, parity * rows, rows)
        else:
            ref = piece(source, parity * rows + way * quarter, quarter)
        sems = right_sem if way == 0 else left_sem
        return remote(ref, sent_ring_sem.at[way, step - 1], sems.at[step - 1], at_rank(along(sign)))

    def cross(offset, way):
        source = along(offset)
        ref = piece(source, parity * rows + way * quarter, quarter)
        index = (offset + length) % length
        return remote(ref, sent_cross_sem.at[way, index], cross_sem.at[way, index], across(1 if way == 0 else -1))

    def cross_arrival(offset, way):
        source = along(offset)
        ref = piece(source, (1 - parity) * rows + way * quarter, quarter)
        index = (offset + length) % length
        return remote(ref, sent_cross_sem.at[way, index], cross_sem.at[way, index], across(1 if way == 0 else -1))

    def to_mate(offset, which):
        source = along(offset)
        index = (offset + length) % length
        start = (parity if which == 0 else 1 - parity) * rows
        return remote(piece(source, start, rows), sent_mate_sem.at[which, index], mate_sem.at[which, index], mate)

    def from_mate(offset, which):
        index = (offset + length) % length
        start = (parity if which == 0 else 1 - parity) * rows
        ref = weight_buf.at[along(offset) * 2 + 1 - core, pl.ds(pl.multiple_of(start, quarter), rows)]
        return remote(ref, sent_mate_sem.at[which, index], mate_sem.at[which, index], mate)

    def offsets(step):
        return [half_way] if step == half_way else [-step, step]

    def serve_ring(step):
        for way in range(2):
            ring_arrival(step, way).wait_recv()
            if step < half_way:
                ring(step + 1, way).start()
        for offset in offsets(step):
            for way in range(2):
                cross(offset, way).start()
            to_mate(offset, 0).start()

    served = set()

    def serve_cross(step):
        served.add(step)
        for offset in offsets(step):
            for way in range(2):
                cross_arrival(offset, way).wait_recv()
            to_mate(offset, 1).start()

    @pl.loop(0, pairs // batch)
    def _(b):
        prepare_quads([b * (batch // 2) + i for i in range(batch // 2)])

        @pl.when(b == 0)
        def _():
            pl.semaphore_wait(barrier, devices - 1 + 3)
            own.wait()
            for way in range(2):
                ring(1, way).start()
            for which in range(2):
                to_mate(0, which).start()

    def head_copy(head, sender, target):
        return pltpu.make_async_remote_copy(
            src_ref=message_buf.at[head], dst_ref=arrive_buf.at[sender], send_sem=sent_sem, recv_sem=message_sem,
            device_id=target, device_id_type=MESH)

    def decay_copy(head, sender, target):
        return pltpu.make_async_remote_copy(
            src_ref=decay_buf.at[head], dst_ref=arrive_decay.at[sender], send_sem=sent_decay_sem,
            recv_sem=decay_sem, device_id=target, device_id_type=MESH)

    @pl.loop(0, pairs // batch)
    def _(b):
        ats = [pl.ds(pl.multiple_of((b * batch + i) * PAIR, PAIR), PAIR) for i in range(batch)]
        messages = transitions(size, ats, v_ref, ops, solved_bufs)
        for i, (first, second) in enumerate(messages):
            message_buf[2 * (b * batch + i)] = first
            message_buf[2 * (b * batch + i) + 1] = second
        count = 2 * batch

        @pl.loop(0, count)
        def _(j):
            head = b * count + lax.rem(me + j, count)

            @pl.when(head != my_head)
            def _():
                head_copy(head, me, {"sp": keeper(head)}).start()
                decay_copy(head, me, {"sp": keeper(head)}).start()

        @pl.when(b == 0)
        def _():
            serve_ring(1)

    arrive_buf[me] = message_buf[my_head]
    arrive_decay[me] = decay_buf[my_head]
    serve_cross(1)
    if half_way > 1:
        serve_ring(2)

    @pl.loop(0, pairs // batch)
    def _(b):
        wavefront([readouts(size, pl.ds(pl.multiple_of((b * batch + i) * PAIR, PAIR), PAIR), v_ref, ops,
                            solved_bufs, local_bufs) for i in range(batch)])

    if half_way > 1:
        serve_cross(2)
    if half_way > 2:
        serve_ring(3)

    others = pl.ds(0, devices - 1)
    pltpu.make_async_copy(arrive_buf.at[others], arrive_buf.at[others], message_sem).wait()
    pltpu.make_async_copy(arrive_decay.at[others], arrive_decay.at[others], decay_sem).wait()

    def back_copy(chunk, head, target):
        return pltpu.make_async_remote_copy(
            src_ref=back_buf.at[chunk], dst_ref=start_buf.at[head], send_sem=sent_back_sem, recv_sem=back_sem.at[head],
            device_id=target, device_id_type=MESH)

    row = iota((HEAD, PAIR), 0)
    lane = iota((HEAD, PAIR), 1)
    lower = lane < HEAD
    marker = jnp.where(lane == row + HEAD, F32(1.0), F32(0.0)).astype(BF16)
    marker = cat([jnp.zeros_like(marker), marker], 0)
    low_tall = iota((PAIR, PAIR), 1) < HEAD
    begin = jnp.where(iota((PAIR, PAIR), 0) == iota((PAIR, PAIR), 1), F32(1.0), F32(0.0))
    begin = jnp.where(low_tall, begin, 0.0)
    per = devices // XDIM
    steps = [[begin] for _ in range(XDIM)]
    for r in range(per):
        for g in range(XDIM):
            if g == XDIM - 1 and r == per - 1:
                continue
            c = g * per + r
            now = steps[g][-1]
            message = arrive_buf[c]
            moved = mm_nt(jnp.where(low_tall, now.astype(BF16), marker), cat([message, jnp.zeros_like(message)], 0))
            steps[g].append(moved + now * arrive_decay[c])

    def put_back(c, state):
        average = jnp.mean(state, axis=0, keepdims=True)
        centred = jnp.where(lower, state - average, 0.0)
        back_buf[c] = (centred[: HEAD // 2] + pltpu.roll(centred[HEAD // 2 :], HEAD, 1)).astype(BF16)

    state = jnp.zeros((HEAD, PAIR), F32)
    for g in range(XDIM):
        high, low = split(state)
        left = cat([jnp.where(lower, high, jnp.zeros_like(high)), jnp.where(lower, low, jnp.zeros_like(low))], 0)
        for r in range(per + 1):
            if g == XDIM - 1 and r == per:
                continue
            both = steps[g][r]
            if r == 0:
                reached = state
            elif g == 0:
                reached = both[HEAD:]
            else:
                moved = mm(left, both.astype(BF16))
                reached = moved[:HEAD] + moved[HEAD:] + both[HEAD:]
            if r < per:
                put_back(g * per + r, reached)
            else:
                state = reached

    @pl.loop(1, devices)
    def _(j):
        chunk = lax.rem(me + j, devices)
        back_copy(chunk, my_head, {"sp": chunk}).start()

    start_buf[my_head] = back_buf[me]

    for step in range(3, half_way):
        serve_cross(step)
        serve_ring(step + 1)

    mean_ones = cat([same_head_ones(PAIR, 1.0 / HEAD)] * 2, 0)
    centring = jnp.where(lane == row + HEAD, F32(1.0 - 1.0 / HEAD), F32(-1.0 / HEAD)).astype(BF16)

    def finish_wait(p):
        for i in range(2):
            head = 2 * p + i

            @pl.when(head != my_head)
            def _():
                back_copy(me, head, {"sp": me}).wait_recv()

    def finish_pair(p):
        at = pl.ds(pl.multiple_of(p * PAIR, PAIR), PAIR)
        wide = pl.ds(pl.multiple_of(p * QUAD, QUAD), QUAD)
        rights = []
        for i in range(2):
            packed = start_buf[2 * p + i]
            rights.append(jnp.where(lower, cat([packed, swap_halves(packed)], 0), centring))
        right = diag2(rights[0], rights[1])
        centred = mm_nt(local_high[:, wide], right) + mm_nt(local_low[:, wide], right)
        yield
        variance = mm(cat(split(centred * centred), 1), mean_ones)
        yield
        mix_buf[:, at] = (centred * lax.rsqrt(variance + 1.0) * gain_ref[:, at]).astype(BF16)

    @pl.loop(0, pairs // batch)
    def _(b):
        for i in range(batch):
            finish_wait(b * batch + i)
        wavefront([finish_pair(b * batch + i) for i in range(batch)])

    def project(offset):
        at = along(offset)
        weight = cat([weight_buf[2 * at], weight_buf[2 * at + 1]], 1)
        out_ref[:, pl.ds(pl.multiple_of(at * QUAD, QUAD), QUAD)] = mm(mix_buf[...], weight).astype(BF16)

    last = [step for step in range(1, half_way + 1) if step not in served]
    early = [offset for step in range(1, half_way) for offset in offsets(step)]
    for offset in [0] + early:
        for which in range(2):
            from_mate(offset, which).wait_recv()
    for step in last:
        serve_cross(step)
    for offset in [0] + early:
        project(offset)
    for which in range(2):
        from_mate(half_way, which).wait_recv()
    project(half_way)

    pltpu.make_async_copy(message_buf.at[others], message_buf.at[others], sent_sem).wait()
    pltpu.make_async_copy(decay_buf.at[others], decay_buf.at[others], sent_decay_sem).wait()
    pltpu.make_async_copy(back_buf.at[others], back_buf.at[others], sent_back_sem).wait()
    for step in range(1, half_way + 1):
        for way in range(2):
            ring(step, way).wait_send()
        for offset in offsets(step):
            for way in range(2):
                cross(offset, way).wait_send()
            for which in range(2):
                to_mate(offset, which).wait_send()
    for which in range(2):
        to_mate(0, which).wait_send()


def per_device(devices, ranks, query_rows, key_rows, value_rows, decay_low, rate_low, decay_up, rate_up,
               decay_base, norm_gain, out_weight):
    size, width = query_rows.shape[1:]
    heads = width // HEAD
    batch = min(8, width // PAIR)
    length = ranks // 2
    half_way = length // 2
    vmem = pl.BlockSpec(memory_space=pltpu.VMEM)
    dma = pltpu.SemaphoreType.DMA
    wide = lambda lanes: pltpu.VMEM((size, lanes), BF16)
    out = pl.pallas_call(
        functools.partial(mixer_kernel, devices, ranks, batch),
        in_specs=[vmem] * 9 + [pl.BlockSpec(memory_space=pl.ANY)],
        out_specs=vmem,
        out_shape=jax.ShapeDtypeStruct((size, out_weight.shape[1] * ranks), BF16),
        scratch_shapes=[wide(width) for _ in range(10)] + [pltpu.VMEM((size, width), F32)] * 2
        + [wide(2 * width) for _ in range(4)] + [wide(width)] + [
            pltpu.VMEM((heads, HEAD, PAIR), BF16),
            pltpu.VMEM((heads, 1, PAIR), F32),
            pltpu.VMEM((devices, HEAD, PAIR), BF16),
            pltpu.VMEM((devices, 1, PAIR), F32),
            pltpu.VMEM((devices, HEAD // 2, PAIR), BF16),
            pltpu.VMEM((heads, HEAD // 2, PAIR), BF16),
            pltpu.VMEM((ranks,) + out_weight.shape, BF16),
            dma, dma, dma((heads,)), dma, dma, dma,
            dma((half_way,)), dma((half_way,)), dma((2, length)), dma((2, length)),
            dma((2, half_way)), dma((2, length)), dma((2, length)), dma,
        ],
        compiler_params=pltpu.CompilerParams(
            collective_id=0, has_side_effects=True, vmem_limit_bytes=60 * 2**20),
        cost_estimate=pl.CostEstimate(flops=10**10, bytes_accessed=10**7, transcendentals=0),
        name="mixer",
    )(query_rows[0], key_rows[0], value_rows[0], decay_low[0], rate_low[0], decay_up, rate_up,
      decay_base[None], norm_gain[None], out_weight)
    return out[None]


def solution(mesh):
    in_specs = (
        P("dp", "sp", None),
        P("dp", "sp", None),
        P("dp", "sp", None),
        P("dp", "sp", None),
        P("dp", "sp", None),
        P(),
        P(),
        P(),
        P(),
        P(None, "dp"),
    )
    return jax.shard_map(
        functools.partial(per_device, mesh.shape["sp"], mesh.shape["dp"]),
        mesh=mesh, in_specs=in_specs, out_specs=P("dp", "sp", None), check_vma=False,
    )
```

```python
import functools
import math

import jax
import jax.numpy as jnp
from jax import lax
from jax.experimental import pallas as pl
from jax.experimental.pallas import tpu as pltpu
from jax.sharding import PartitionSpec as P

HEAD = 64
PAIR = 2 * HEAD
QUAD = 2 * PAIR
XDIM = 4

F32 = jnp.float32
BF16 = jnp.bfloat16
MESH = pl.DeviceIdType.MESH


def mm(left, right):
    return lax.dot_general(left, right, (((1,), (0,)), ((), ())), preferred_element_type=F32)


def mm_nt(left, right):
    return lax.dot_general(left, right, (((1,), (1,)), ((), ())), preferred_element_type=F32)


def mm_tn(left, right):
    return lax.dot_general(left, right, (((0,), (0,)), ((), ())), preferred_element_type=F32)


def split(x):
    high = x.astype(BF16)
    return high, (x - high.astype(F32)).astype(BF16)


def iota(shape, dim):
    return lax.broadcasted_iota(jnp.int32, shape, dim)


def cat(parts, axis):
    return jnp.concatenate(parts, axis=axis)


def diag2(a, b):
    return cat([cat([a, jnp.zeros_like(b)], 1), cat([jnp.zeros_like(a), b], 1)], 0)


def swap_halves(x):
    return pltpu.roll(x.astype(F32), HEAD, 1).astype(x.dtype)


def low_half(shape):
    return lax.rem(iota(shape, 1), PAIR) < HEAD


def stack_pair(x):
    here = low_half(x.shape)
    zero = jnp.zeros_like(x)
    return cat([jnp.where(here, x, zero), jnp.where(here, zero, x)], 0)


def same_head_ones(width, scale):
    same = (iota((width, width), 0) // HEAD) == (iota((width, width), 1) // HEAD)
    return jnp.where(same, F32(scale), F32(0.0)).astype(BF16)


def put_split(refs, at, x):
    high, low = split(x)
    refs[0][:, at] = high
    refs[1][:, at] = low


def wavefront(works):
    running = []
    waiting = list(works)
    while waiting or running:
        if waiting:
            running.append(waiting.pop(0))
        running = [work for work in running if next(work, 0) is None]


def prepare(size, at, q_ref, k_ref, squashed, rate_low, dup_ref, rup_ref, base_ref, ops, decay_buf, pair):
    middle = size // 2
    upto = jnp.where(iota((size, size), 0) >= iota((size, size), 1), F32(1.0), F32(0.0)).astype(BF16)
    upto = cat([upto, upto], 1)
    decay_pre = mm(squashed, dup_ref[:, at])
    rate_pre = mm(rate_low, rup_ref[:, at])
    yield
    decay_pre = (base_ref[:, at] + decay_pre).astype(BF16).astype(F32)
    rate_pre = rate_pre.astype(BF16).astype(F32)
    log_decay = -math.exp(-0.5) / (1.0 + jnp.exp(-decay_pre))
    rate = 1.0 / (1.0 + jnp.exp(-rate_pre))
    running = mm(upto, cat(split(log_decay), 0))
    k = k_ref[:, at].astype(F32)
    norm = mm(cat(split(k * k), 1), cat([same_head_ones(QUAD, 1.0)] * 2, 0))
    yield
    centre = running[middle : middle + 1]
    final = running[size - 1 :]
    shifted = running - centre
    ahead = jnp.exp(shifted)
    before = jnp.exp(shifted - log_decay)
    behind = jnp.exp(-shifted)
    at_centre = jnp.exp(centre)
    at_end = jnp.exp(final - centre)
    q = q_ref[:, at].astype(F32)
    unit = k * lax.rsqrt(1.0 + norm)
    erase_from = unit * before
    read_mid = q * ahead
    key_to = k * behind
    erase_to = -(unit * rate) * behind
    put_split(ops["from"], at, erase_from)
    put_split(ops["read"], at, read_mid)
    put_split(ops["key"], at, key_to)
    put_split(ops["erase"], at, erase_to)
    ops["from_start"][:, at] = erase_from * at_centre
    ops["read_start"][:, at] = read_mid * at_centre
    ops["key_end"][:, at] = (key_to * at_end).astype(BF16)
    ops["erase_end"][:, at] = (erase_to * at_end).astype(BF16)
    decays = jnp.exp(final)
    for i in range(2):
        here = decays[:, i * PAIR : (i + 1) * PAIR]
        decay_buf[2 * (pair + i)] = here
        decay_buf[2 * (pair + i) + 1] = pltpu.roll(here, HEAD, 1)


def by_head(x):
    return diag2(x[:, :PAIR], x[:, PAIR:])


def raw_grid(left, ops, at):
    high, low = (stack_pair(ref[:, at]) for ref in left)
    right = cat([ops["key"][0][:, at], ops["erase"][0][:, at]], 0)
    rest = cat([ops["key"][1][:, at], ops["erase"][1][:, at]], 0)
    return mm_nt(cat([high, low], 1), cat([right, right], 1)) + mm_nt(high, rest)


def grid_parts(size, grid, keep):
    part = lambda i, j: jnp.where(keep, grid[i * size : (i + 1) * size, j * size : (j + 1) * size], 0.0)
    return split(cat([part(0, 0), part(1, 0)], 1)), split(cat([part(0, 1), part(1, 1)], 1))


def inverses(splits, size):
    negs = [high for high, _ in splits]
    row = iota((size, PAIR * 2), 0)
    col = lax.rem(iota((size, PAIR * 2), 1), PAIR)
    eye = jnp.where(row == col, F32(1.0), F32(0.0)).astype(BF16)
    found = None
    block = 1
    while block < size:
        pick = (row // (2 * block) == col // (2 * block)) & (row // block != col // block) & (row > col)
        pieces = [jnp.where(pick, n, jnp.zeros_like(n)) for n in negs]
        if found is None:
            found = [eye + p for p in pieces]
        elif block < 16:
            right = [mm(p, by_head(x)).astype(BF16) for p, x in zip(pieces, found)]
            found = [x + mm(x, by_head(y)).astype(BF16) for x, y in zip(found, right)]
        else:
            starts = list(range(block, size, 2 * block))
            take = lambda m: cat([m[s : s + block] for s in starts], 0) if len(starts) > 1 else m[block:]
            right = [mm(take(p), by_head(x)).astype(BF16) for p, x in zip(pieces, found)]
            blank = jnp.zeros((block, 2 * PAIR), BF16)
            spread = lambda m: cat(
                [part for j in range(len(starts)) for part in (blank, m[j * block : (j + 1) * block])], 0)
            right = [spread(y) for y in right]
            step = [mm(take(x), by_head(y)).astype(BF16) for x, y in zip(found, right)]
            found = [x + spread(t) for x, t in zip(found, step)]
        block *= 2
    left = [mm(high, by_head(x)) + mm(low, by_head(x)) for (high, low), x in zip(splits, found)]
    left = [((eye - x).astype(F32) + r).astype(BF16) for x, r in zip(found, left)]
    return [(x, mm(x, by_head(r)).astype(BF16)) for x, r in zip(found, left)]


def low_part(x):
    return jnp.where(low_half(x.shape), x, jnp.zeros_like(x))


def high_part(x):
    return jnp.where(low_half(x.shape), jnp.zeros_like(x), x)


def transitions(size, ats, v_ref, ops, solved_bufs, pause):
    strict = iota((size, size), 0) > iota((size, size), 1)
    negs, sides = [], []

    def front(at):
        grid = raw_grid(ops["from"], ops, at)
        yield
        keys, neg = grid_parts(size, grid, strict)
        negs.append(neg)
        v = v_ref[:, at]
        values = diag2(high_part(swap_halves(v)), high_part(v))
        carried = mm(keys[0], values) + mm(keys[1], values)
        yield
        base = ops["from_start"][:, at]
        lows = cat([low_part(base), low_part(swap_halves(base))], 1)
        sides.append(split(lows + carried))

    wavefront([front(at) for at in ats])
    found = inverses(negs, size)
    pause()
    solved = [split(mm(x[0], by_head(side[0])) + mm(x[0], by_head(side[1])) + mm(x[1], by_head(side[0])))
              for x, side in zip(found, sides)]
    made = []
    for at, parts in zip(ats, solved):
        wide = pl.ds(pl.multiple_of(2 * at.start, QUAD), QUAD)
        solved_bufs[0][:, wide] = parts[0]
        solved_bufs[1][:, wide] = parts[1]
        v = v_ref[:, at]
        ends = cat([ops["erase_end"][:, at], ops["key_end"][:, at]], 0)
        values = cat([high_part(swap_halves(v)), high_part(v)], 1)
        made.append(mm_tn(ends, cat([parts[0], values], 0)))
    return [(m[:HEAD, :PAIR].astype(BF16), m[HEAD:, PAIR:].astype(BF16)) for m in made]


def readouts(size, at, v_ref, ops, solved_bufs, local_bufs):
    within = iota((size, size), 0) >= iota((size, size), 1)
    grid = raw_grid(ops["read"], ops, at)
    yield
    keys, erases = grid_parts(size, grid, within)
    left = [cat([e[:, :PAIR], k[:, :PAIR], e[:, PAIR:], k[:, PAIR:]], 1) for k, e in zip(keys, erases)]
    wide = pl.ds(pl.multiple_of(2 * at.start, QUAD), QUAD)
    solved = solved_bufs[0][:, wide]
    v = v_ref[:, at]
    right = diag2(cat([solved[:, :PAIR], high_part(swap_halves(v))], 0), cat([solved[:, PAIR:], high_part(v)], 0))
    taken = mm(left[0], right) + mm(left[1], right) + mm(erases[0], by_head(solved_bufs[1][:, wide]))
    yield
    base = ops["read_start"][:, at]
    lows = cat([low_part(base), low_part(swap_halves(base))], 1)
    put_split(local_bufs, wide, lows + taken)


def mixer_kernel(devices, ranks, batch,
                 q_in, k_in, v_in, low_ref, rate_ref, dup_in, rup_in, base_ref, gain_ref, w_ref,
                 out_ref,
                 q_ref, k_ref, v_ref, dup_ref, rup_ref, load_sem,
                 from_high, from_low, read_high, read_low, key_high, key_low, erase_high, erase_low,
                 key_end, erase_end, from_start, read_start,
                 solved_high, solved_low, local_high, local_low, mix_buf,
                 message_buf, decay_buf, arrive_buf, arrive_decay, back_buf, start_buf, weight_buf,
                 message_sem, decay_sem, back_sem, sent_sem, sent_decay_sem, sent_back_sem,
                 ring_sem, cross_sem, mate_sem, whole_sem, sent_ring_sem, sent_cross_sem, sent_mate_sem, sent_whole_sem,
                 own_sem):
    size, width = q_ref.shape
    pairs = width // PAIR
    ops = {"from": (from_high, from_low), "read": (read_high, read_low), "key": (key_high, key_low),
           "erase": (erase_high, erase_low), "key_end": key_end, "erase_end": erase_end,
           "from_start": from_start, "read_start": read_start}
    solved_bufs = (solved_high, solved_low)
    local_bufs = (local_high, local_low)
    me = lax.axis_index("sp")
    rank = lax.axis_index("dp")
    length = ranks // 2
    half_way = length // 2
    core = lax.rem(rank, 2)
    line = rank // 2
    along = lambda step: lax.rem(line + step + length, length)
    at_rank = lambda row: {"dp": row * 2 + core}
    mate = {"dp": rank + 1 - 2 * core}
    x = lax.rem(me, XDIM)
    across = lambda step: {"sp": me - x + lax.rem(x + step + XDIM, XDIM)}
    parity = lax.rem(x, 2)
    rows = width // 2
    quarter = rows // 2

    planes = devices // XDIM
    plane = me // XDIM
    my_head = lax.rem(x + planes * XDIM - plane, XDIM) * planes + plane

    def keeper(head):
        place = lax.rem(head, planes)
        return place * XDIM + lax.rem(place + head // planes, XDIM)

    own = pltpu.make_async_copy(w_ref, weight_buf.at[rank], own_sem)
    own.start()
    loads = [pltpu.make_async_copy(source, target, load_sem.at[i]) for i, (source, target) in enumerate(
        ((dup_in, dup_ref), (rup_in, rup_ref), (k_in, k_ref), (q_in, q_ref), (v_in, v_ref)))]
    for load in loads:
        load.start()

    barrier = pltpu.get_barrier_semaphore()

    @pl.loop(1, devices)
    def _(j):
        pl.semaphore_signal(barrier, inc=1, device_id={"sp": lax.rem(me + j, devices)}, device_id_type=MESH)

    for target in (at_rank(along(1)), at_rank(along(-1)), mate):
        pl.semaphore_signal(barrier, inc=1, device_id=target, device_id_type=MESH)

    last = 2 * half_way - 2

    def quarters(source, kind, start):
        return weight_buf.at[source * 2 + kind, pl.ds(pl.multiple_of(start, quarter), quarter)]

    def remote(ref, sem_out, sem_in, target):
        return pltpu.make_async_remote_copy(
            src_ref=ref, dst_ref=ref, send_sem=sem_out, recv_sem=sem_in, device_id=target, device_id_type=MESH)

    def turn(way):
        return 1 if way == 0 else -1

    def part_of(n, way):
        half = lax.rem(n, 2)
        return half if way == 0 else 1 - half

    def ring(n, way, hops):
        source = along(-turn(way) * hops)
        ref = quarters(source, core, parity * rows + part_of(n, way) * quarter)
        return remote(ref, sent_ring_sem.at[way, n], ring_sem.at[way, n], at_rank(along(turn(way))))

    def ring_out(n, way):
        return ring(n, way, n // 2)

    def ring_in(n, way):
        return ring(n, way, n // 2 + 1)

    def cross(n, way, own_side):
        part = part_of(n, way)
        side = parity if own_side else 1 - parity
        ref = quarters(along(-turn(way) * (n // 2 + 1)), core, side * rows + part * quarter)
        return remote(ref, sent_cross_sem.at[way, n], cross_sem.at[way, n], across(1 - 2 * part))

    def to_mate(n, way, own_side, kind):
        side = parity if own_side else 1 - parity
        ref = quarters(along(-turn(way) * (n // 2 + 1)), kind, side * rows + part_of(n, way) * quarter)
        which = 0 if own_side else 1
        return remote(ref, sent_mate_sem.at[way, which, n], mate_sem.at[way, which, n], mate)

    def whole_to_mate(kind):
        return remote(weight_buf.at[line * 2 + kind], sent_whole_sem, whole_sem, mate)

    def serve_ring(n):
        for way in range(2):
            ring_in(n, way).wait_recv()

            @pl.when(n + 2 <= last)
            def _():
                ring_out(n + 2, way).start()

        for way in range(2):
            cross(n, way, True).start()
            to_mate(n, way, True, core).start()

    def serve_cross(n):
        for way in range(2):
            cross(n, way, False).wait_recv()
            to_mate(n, way, False, core).start()

    pl.semaphore_wait(barrier, devices - 1 + 3)
    own.wait()
    for n in range(2 if half_way > 1 else 1):
        for way in range(2):
            ring_out(n, way).start()
    whole_to_mate(core).start()

    rounds = pairs // batch

    def serve(n):
        @pl.when(n <= last)
        def _():
            serve_ring(n)

            @pl.when(n >= 2)
            def _():
                serve_cross(n - 2)

    for load in loads:
        load.wait()
    squashed = jnp.tanh(low_ref[...].astype(F32)).astype(BF16)
    rate_low = rate_ref[...]

    @pl.loop(0, rounds)
    def _(b):
        wavefront([prepare(size, pl.ds(pl.multiple_of((b * (batch // 2) + i) * QUAD, QUAD), QUAD), q_ref, k_ref,
                           squashed, rate_low, dup_ref, rup_ref, base_ref, ops, decay_buf,
                           2 * (b * (batch // 2) + i)) for i in range(batch // 2)])

    def head_copy(head, sender, target):
        return pltpu.make_async_remote_copy(
            src_ref=message_buf.at[head], dst_ref=arrive_buf.at[sender], send_sem=sent_sem, recv_sem=message_sem,
            device_id=target, device_id_type=MESH)

    def decay_copy(head, sender, target):
        return pltpu.make_async_remote_copy(
            src_ref=decay_buf.at[head], dst_ref=arrive_decay.at[sender], send_sem=sent_decay_sem,
            recv_sem=decay_sem, device_id=target, device_id_type=MESH)

    @pl.loop(0, pairs // batch)
    def _(b):
        ats = [pl.ds(pl.multiple_of((b * batch + i) * PAIR, PAIR), PAIR) for i in range(batch)]
        messages = transitions(size, ats, v_ref, ops, solved_bufs, lambda: serve(2 * b))
        for i, (first, second) in enumerate(messages):
            message_buf[2 * (b * batch + i)] = first
            message_buf[2 * (b * batch + i) + 1] = second
        count = 2 * batch

        @pl.loop(0, count)
        def _(j):
            head = b * count + lax.rem(me + j, count)

            @pl.when(head != my_head)
            def _():
                head_copy(head, me, {"sp": keeper(head)}).start()
                decay_copy(head, me, {"sp": keeper(head)}).start()

        serve(2 * b + 1)

    arrive_buf[me] = message_buf[my_head]
    arrive_decay[me] = decay_buf[my_head]
    @pl.loop(0, pairs // batch)
    def _(b):
        wavefront([readouts(size, pl.ds(pl.multiple_of((b * batch + i) * PAIR, PAIR), PAIR), v_ref, ops,
                            solved_bufs, local_bufs) for i in range(batch)])
        serve(2 * rounds + b)

    others = pl.ds(0, devices - 1)
    pltpu.make_async_copy(arrive_buf.at[others], arrive_buf.at[others], message_sem).wait()
    pltpu.make_async_copy(arrive_decay.at[others], arrive_decay.at[others], decay_sem).wait()

    def back_copy(chunk, head, target):
        return pltpu.make_async_remote_copy(
            src_ref=back_buf.at[chunk], dst_ref=start_buf.at[head], send_sem=sent_back_sem, recv_sem=back_sem.at[head],
            device_id=target, device_id_type=MESH)

    row = iota((HEAD, PAIR), 0)
    lane = iota((HEAD, PAIR), 1)
    lower = lane < HEAD
    marker = jnp.where(lane == row + HEAD, F32(1.0), F32(0.0)).astype(BF16)
    marker = cat([jnp.zeros_like(marker), marker], 0)
    low_tall = iota((PAIR, PAIR), 1) < HEAD
    begin = jnp.where(iota((PAIR, PAIR), 0) == iota((PAIR, PAIR), 1), F32(1.0), F32(0.0))
    begin = jnp.where(low_tall, begin, 0.0)
    per = devices // XDIM
    steps = [[begin] for _ in range(XDIM)]
    for r in range(per):
        for g in range(XDIM):
            if g == XDIM - 1 and r == per - 1:
                continue
            c = g * per + r
            now = steps[g][-1]
            message = arrive_buf[c]
            moved = mm_nt(jnp.where(low_tall, now.astype(BF16), marker), cat([message, jnp.zeros_like(message)], 0))
            steps[g].append(moved + now * arrive_decay[c])

    def put_back(c, state):
        average = jnp.mean(state, axis=0, keepdims=True)
        centred = jnp.where(lower, state - average, 0.0)
        back_buf[c] = (centred[: HEAD // 2] + pltpu.roll(centred[HEAD // 2 :], HEAD, 1)).astype(BF16)

    state = jnp.zeros((HEAD, PAIR), F32)
    for g in range(XDIM):
        high, low = split(state)
        left = cat([jnp.where(lower, high, jnp.zeros_like(high)), jnp.where(lower, low, jnp.zeros_like(low))], 0)
        for r in range(per + 1):
            if g == XDIM - 1 and r == per:
                continue
            both = steps[g][r]
            if r == 0:
                reached = state
            elif g == 0:
                reached = both[HEAD:]
            else:
                moved = mm(left, both.astype(BF16))
                reached = moved[:HEAD] + moved[HEAD:] + both[HEAD:]
            if r < per:
                put_back(g * per + r, reached)
            else:
                state = reached

    @pl.loop(1, devices)
    def _(j):
        chunk = lax.rem(me + j, devices)
        back_copy(chunk, my_head, {"sp": chunk}).start()

    start_buf[my_head] = back_buf[me]

    seen = min(3 * rounds, last + 1)
    for n in range(seen, last + 1):
        serve_ring(n)
    crossed = max(seen - 2, 0)
    for n in range(crossed, last - 1):
        serve_cross(n)
    crossed = max(crossed, last - 1)

    mean_ones = cat([same_head_ones(PAIR, 1.0 / HEAD)] * 2, 0)
    centring = jnp.where(lane == row + HEAD, F32(1.0 - 1.0 / HEAD), F32(-1.0 / HEAD)).astype(BF16)

    def finish_wait(p):
        for i in range(2):
            head = 2 * p + i

            @pl.when(head != my_head)
            def _():
                back_copy(me, head, {"sp": me}).wait_recv()

    def finish_pair(p):
        at = pl.ds(pl.multiple_of(p * PAIR, PAIR), PAIR)
        wide = pl.ds(pl.multiple_of(p * QUAD, QUAD), QUAD)
        rights = []
        for i in range(2):
            packed = start_buf[2 * p + i]
            rights.append(jnp.where(lower, cat([packed, swap_halves(packed)], 0), centring))
        right = diag2(rights[0], rights[1])
        centred = mm_nt(local_high[:, wide], right) + mm_nt(local_low[:, wide], right)
        yield
        variance = mm(cat(split(centred * centred), 1), mean_ones)
        yield
        mix_buf[:, at] = (centred * lax.rsqrt(variance + 1.0) * gain_ref[:, at]).astype(BF16)

    @pl.loop(0, pairs // batch)
    def _(b):
        for i in range(batch):
            finish_wait(b * batch + i)
        wavefront([finish_pair(b * batch + i) for i in range(batch)])

    def project(offset):
        at = along(offset)
        weight = cat([weight_buf[2 * at], weight_buf[2 * at + 1]], 1)
        out_ref[:, pl.ds(pl.multiple_of(at * QUAD, QUAD), QUAD)] = mm(mix_buf[...], weight).astype(BF16)

    for n in range(crossed, last + 1):
        serve_cross(n)
    whole_to_mate(1 - core).wait_recv()
    project(0)
    for n in range(last + 1):
        for way in range(2):
            for own_side in (True, False):
                to_mate(n, way, own_side, 1 - core).wait_recv()
    for offset in [o for step in range(1, half_way) for o in (-step, step)] + [half_way]:
        project(offset)

    pltpu.make_async_copy(message_buf.at[others], message_buf.at[others], sent_sem).wait()
    pltpu.make_async_copy(decay_buf.at[others], decay_buf.at[others], sent_decay_sem).wait()
    pltpu.make_async_copy(back_buf.at[others], back_buf.at[others], sent_back_sem).wait()
    whole_to_mate(core).wait_send()

    @pl.loop(0, last + 1)
    def _(n):
        for way in range(2):
            ring_out(n, way).wait_send()
            for own_side in (True, False):
                to_mate(n, way, own_side, core).wait_send()
            cross(n, way, True).wait_send()


def per_device(devices, ranks, query_rows, key_rows, value_rows, decay_low, rate_low, decay_up, rate_up,
               decay_base, norm_gain, out_weight):
    size, width = query_rows.shape[1:]
    heads = width // HEAD
    batch = min(8, width // PAIR)
    length = ranks // 2
    pieces = 2 * (length // 2) - 1
    anywhere = pl.BlockSpec(memory_space=pl.ANY)
    vmem = pl.BlockSpec(memory_space=pltpu.VMEM)
    dma = pltpu.SemaphoreType.DMA
    wide = lambda lanes: pltpu.VMEM((size, lanes), BF16)
    out = pl.pallas_call(
        functools.partial(mixer_kernel, devices, ranks, batch),
        in_specs=[anywhere] * 3 + [vmem] * 2 + [anywhere] * 2 + [vmem] * 2 + [anywhere],
        out_specs=vmem,
        out_shape=jax.ShapeDtypeStruct((size, out_weight.shape[1] * ranks), BF16),
        scratch_shapes=[wide(width)] * 3 + [pltpu.VMEM(decay_up.shape, BF16)] * 2 + [dma((5,))]
        + [wide(width) for _ in range(10)] + [pltpu.VMEM((size, width), F32)] * 2
        + [wide(2 * width) for _ in range(4)] + [wide(width)] + [
            pltpu.VMEM((heads, HEAD, PAIR), BF16),
            pltpu.VMEM((heads, 1, PAIR), F32),
            pltpu.VMEM((devices, HEAD, PAIR), BF16),
            pltpu.VMEM((devices, 1, PAIR), F32),
            pltpu.VMEM((devices, HEAD // 2, PAIR), BF16),
            pltpu.VMEM((heads, HEAD // 2, PAIR), BF16),
            pltpu.VMEM((ranks,) + out_weight.shape, BF16),
            dma, dma, dma((heads,)), dma, dma, dma,
            dma((2, pieces)), dma((2, pieces)), dma((2, 2, pieces)), dma,
            dma((2, pieces)), dma((2, pieces)), dma((2, 2, pieces)), dma, dma,
        ],
        compiler_params=pltpu.CompilerParams(
            collective_id=0, has_side_effects=True, vmem_limit_bytes=60 * 2**20),
        cost_estimate=pl.CostEstimate(flops=10**10, bytes_accessed=10**7, transcendentals=0),
        name="mixer",
    )(query_rows[0], key_rows[0], value_rows[0], decay_low[0], rate_low[0], decay_up, rate_up,
      decay_base[None], norm_gain[None], out_weight)
    return out[None]


def solution(mesh):
    in_specs = (
        P("dp", "sp", None),
        P("dp", "sp", None),
        P("dp", "sp", None),
        P("dp", "sp", None),
        P("dp", "sp", None),
        P(),
        P(),
        P(),
        P(),
        P(None, "dp"),
    )
    return jax.shard_map(
        functools.partial(per_device, mesh.shape["sp"], mesh.shape["dp"]),
        mesh=mesh, in_specs=in_specs, out_specs=P("dp", "sp", None), check_vma=False,
    )
```

```python
import functools
import math

import jax
import jax.numpy as jnp
from jax import lax
from jax.experimental import pallas as pl
from jax.experimental.pallas import tpu as pltpu
from jax.sharding import PartitionSpec as P

HEAD = 64
PAIR = 2 * HEAD
QUAD = 2 * PAIR
XDIM = 4

F32 = jnp.float32
BF16 = jnp.bfloat16
MESH = pl.DeviceIdType.MESH


def mm(left, right):
    return lax.dot_general(left, right, (((1,), (0,)), ((), ())), preferred_element_type=F32)


def mm_nt(left, right):
    return lax.dot_general(left, right, (((1,), (1,)), ((), ())), preferred_element_type=F32)


def mm_tn(left, right):
    return lax.dot_general(left, right, (((0,), (0,)), ((), ())), preferred_element_type=F32)


def split(x):
    high = x.astype(BF16)
    return high, (x - high.astype(F32)).astype(BF16)


def iota(shape, dim):
    return lax.broadcasted_iota(jnp.int32, shape, dim)


def cat(parts, axis):
    return jnp.concatenate(parts, axis=axis)


def diag2(a, b):
    return cat([cat([a, jnp.zeros_like(b)], 1), cat([jnp.zeros_like(a), b], 1)], 0)


def swap_halves(x):
    return pltpu.roll(x.astype(F32), HEAD, 1).astype(x.dtype)


def low_half(shape):
    return lax.rem(iota(shape, 1), PAIR) < HEAD


def stack_pair(x):
    here = low_half(x.shape)
    zero = jnp.zeros_like(x)
    return cat([jnp.where(here, x, zero), jnp.where(here, zero, x)], 0)


def same_head_ones(width, scale):
    same = (iota((width, width), 0) // HEAD) == (iota((width, width), 1) // HEAD)
    return jnp.where(same, F32(scale), F32(0.0)).astype(BF16)


def put_split(refs, at, x):
    high, low = split(x)
    refs[0][:, at] = high
    refs[1][:, at] = low


def wavefront(works):
    running = []
    waiting = list(works)
    while waiting or running:
        if waiting:
            running.append(waiting.pop(0))
        running = [work for work in running if next(work, 0) is None]


def prepare(size, at, q_ref, k_ref, squashed, rate_low, dup_ref, rup_ref, base_ref, ops, decay_buf, pair):
    middle = size // 2
    upto = jnp.where(iota((size, size), 0) >= iota((size, size), 1), F32(1.0), F32(0.0)).astype(BF16)
    upto = cat([upto, upto], 1)
    decay_pre = mm(squashed, dup_ref[:, at])
    rate_pre = mm(rate_low, rup_ref[:, at])
    yield
    decay_pre = (base_ref[:, at] + decay_pre).astype(BF16).astype(F32)
    rate_pre = rate_pre.astype(BF16).astype(F32)
    log_decay = -math.exp(-0.5) / (1.0 + jnp.exp(-decay_pre))
    rate = 1.0 / (1.0 + jnp.exp(-rate_pre))
    running = mm(upto, cat(split(log_decay), 0))
    k = k_ref[:, at].astype(F32)
    norm = mm(cat(split(k * k), 1), cat([same_head_ones(QUAD, 1.0)] * 2, 0))
    yield
    centre = running[middle : middle + 1]
    final = running[size - 1 :]
    shifted = running - centre
    ahead = jnp.exp(shifted)
    before = jnp.exp(shifted - log_decay)
    behind = jnp.exp(-shifted)
    at_centre = jnp.exp(centre)
    at_end = jnp.exp(final - centre)
    q = q_ref[:, at].astype(F32)
    unit = k * lax.rsqrt(1.0 + norm)
    erase_from = unit * before
    read_mid = q * ahead
    key_to = k * behind
    erase_to = -(unit * rate) * behind
    put_split(ops["from"], at, erase_from)
    put_split(ops["read"], at, read_mid)
    put_split(ops["key"], at, key_to)
    put_split(ops["erase"], at, erase_to)
    ops["from_start"][:, at] = erase_from * at_centre
    ops["read_start"][:, at] = read_mid * at_centre
    ops["key_end"][:, at] = (key_to * at_end).astype(BF16)
    ops["erase_end"][:, at] = (erase_to * at_end).astype(BF16)
    decays = jnp.exp(final)
    for i in range(2):
        here = decays[:, i * PAIR : (i + 1) * PAIR]
        decay_buf[2 * (pair + i)] = here
        decay_buf[2 * (pair + i) + 1] = pltpu.roll(here, HEAD, 1)


def by_head(x):
    return diag2(x[:, :PAIR], x[:, PAIR:])


def raw_grid(left, ops, at):
    high, low = (stack_pair(ref[:, at]) for ref in left)
    right = cat([ops["key"][0][:, at], ops["erase"][0][:, at]], 0)
    rest = cat([ops["key"][1][:, at], ops["erase"][1][:, at]], 0)
    return mm_nt(cat([high, low], 1), cat([right, right], 1)) + mm_nt(high, rest)


def grid_parts(size, grid, keep):
    part = lambda i, j: jnp.where(keep, grid[i * size : (i + 1) * size, j * size : (j + 1) * size], 0.0)
    return split(cat([part(0, 0), part(1, 0)], 1)), split(cat([part(0, 1), part(1, 1)], 1))


def inverses(splits, size):
    negs = [high for high, _ in splits]
    row = iota((size, PAIR * 2), 0)
    col = lax.rem(iota((size, PAIR * 2), 1), PAIR)
    eye = jnp.where(row == col, F32(1.0), F32(0.0)).astype(BF16)
    found = None
    block = 1
    while block < size:
        pick = (row // (2 * block) == col // (2 * block)) & (row // block != col // block) & (row > col)
        pieces = [jnp.where(pick, n, jnp.zeros_like(n)) for n in negs]
        if found is None:
            found = [eye + p for p in pieces]
        elif block < 16:
            right = [mm(p, by_head(x)).astype(BF16) for p, x in zip(pieces, found)]
            found = [x + mm(x, by_head(y)).astype(BF16) for x, y in zip(found, right)]
        else:
            starts = list(range(block, size, 2 * block))
            take = lambda m: cat([m[s : s + block] for s in starts], 0) if len(starts) > 1 else m[block:]
            right = [mm(take(p), by_head(x)).astype(BF16) for p, x in zip(pieces, found)]
            blank = jnp.zeros((block, 2 * PAIR), BF16)
            spread = lambda m: cat(
                [part for j in range(len(starts)) for part in (blank, m[j * block : (j + 1) * block])], 0)
            right = [spread(y) for y in right]
            step = [mm(take(x), by_head(y)).astype(BF16) for x, y in zip(found, right)]
            found = [x + spread(t) for x, t in zip(found, step)]
        block *= 2
    left = [mm(high, by_head(x)) + mm(low, by_head(x)) for (high, low), x in zip(splits, found)]
    left = [((eye - x).astype(F32) + r).astype(BF16) for x, r in zip(found, left)]
    return [(x, mm(x, by_head(r)).astype(BF16)) for x, r in zip(found, left)]


def low_part(x):
    return jnp.where(low_half(x.shape), x, jnp.zeros_like(x))


def high_part(x):
    return jnp.where(low_half(x.shape), jnp.zeros_like(x), x)


def transitions(size, ats, v_ref, ops, solved_bufs, pause):
    strict = iota((size, size), 0) > iota((size, size), 1)
    negs, sides = [], []

    def front(at):
        grid = raw_grid(ops["from"], ops, at)
        yield
        keys, neg = grid_parts(size, grid, strict)
        negs.append(neg)
        v = v_ref[:, at]
        values = diag2(high_part(swap_halves(v)), high_part(v))
        carried = mm(keys[0], values) + mm(keys[1], values)
        yield
        base = ops["from_start"][:, at]
        lows = cat([low_part(base), low_part(swap_halves(base))], 1)
        sides.append(split(lows + carried))

    wavefront([front(at) for at in ats])
    found = inverses(negs, size)
    pause()
    solved = [split(mm(x[0], by_head(side[0])) + mm(x[0], by_head(side[1])) + mm(x[1], by_head(side[0])))
              for x, side in zip(found, sides)]
    made = []
    for at, parts in zip(ats, solved):
        wide = pl.ds(pl.multiple_of(2 * at.start, QUAD), QUAD)
        solved_bufs[0][:, wide] = parts[0]
        solved_bufs[1][:, wide] = parts[1]
        v = v_ref[:, at]
        ends = cat([ops["erase_end"][:, at], ops["key_end"][:, at]], 0)
        values = cat([high_part(swap_halves(v)), high_part(v)], 1)
        made.append(mm_tn(ends, cat([parts[0], values], 0)))
    return [(m[:HEAD, :PAIR].astype(BF16), m[HEAD:, PAIR:].astype(BF16)) for m in made]


def readouts(size, at, v_ref, ops, solved_bufs, local_bufs):
    within = iota((size, size), 0) >= iota((size, size), 1)
    grid = raw_grid(ops["read"], ops, at)
    yield
    keys, erases = grid_parts(size, grid, within)
    left = [cat([e[:, :PAIR], k[:, :PAIR], e[:, PAIR:], k[:, PAIR:]], 1) for k, e in zip(keys, erases)]
    wide = pl.ds(pl.multiple_of(2 * at.start, QUAD), QUAD)
    solved = solved_bufs[0][:, wide]
    v = v_ref[:, at]
    right = diag2(cat([solved[:, :PAIR], high_part(swap_halves(v))], 0), cat([solved[:, PAIR:], high_part(v)], 0))
    taken = mm(left[0], right) + mm(left[1], right) + mm(erases[0], by_head(solved_bufs[1][:, wide]))
    yield
    base = ops["read_start"][:, at]
    lows = cat([low_part(base), low_part(swap_halves(base))], 1)
    put_split(local_bufs, wide, lows + taken)


def mixer_kernel(devices, ranks, batch,
                 q_in, k_in, v_in, low_ref, rate_ref, dup_in, rup_in, base_ref, gain_ref, w_ref,
                 out_ref,
                 q_ref, k_ref, v_ref, dup_ref, rup_ref, load_sem,
                 from_high, from_low, read_high, read_low, key_high, key_low, erase_high, erase_low,
                 key_end, erase_end, from_start, read_start,
                 solved_high, solved_low, local_high, local_low, mix_buf,
                 message_buf, decay_buf, arrive_buf, arrive_decay, back_buf, start_buf, weight_buf,
                 message_sem, decay_sem, back_sem, sent_sem, sent_decay_sem, sent_back_sem,
                 ring_sem, cross_sem, mate_sem, whole_sem, sent_ring_sem, sent_cross_sem, sent_mate_sem, sent_whole_sem,
                 own_sem):
    size, width = q_ref.shape
    pairs = width // PAIR
    ops = {"from": (from_high, from_low), "read": (read_high, read_low), "key": (key_high, key_low),
           "erase": (erase_high, erase_low), "key_end": key_end, "erase_end": erase_end,
           "from_start": from_start, "read_start": read_start}
    solved_bufs = (solved_high, solved_low)
    local_bufs = (local_high, local_low)
    me = lax.axis_index("sp")
    rank = lax.axis_index("dp")
    length = ranks // 2
    half_way = length // 2
    core = lax.rem(rank, 2)
    line = rank // 2
    along = lambda step: lax.rem(line + step + length, length)
    at_rank = lambda row: {"dp": row * 2 + core}
    mate = {"dp": rank + 1 - 2 * core}
    x = lax.rem(me, XDIM)
    across = lambda step: {"sp": me - x + lax.rem(x + step + XDIM, XDIM)}
    parity = lax.rem(x, 2)
    rows = width // 2
    quarter = rows // 2

    planes = devices // XDIM
    plane = me // XDIM
    my_head = lax.rem(x + planes * XDIM - plane, XDIM) * planes + plane

    def keeper(head):
        place = lax.rem(head, planes)
        return place * XDIM + lax.rem(place + head // planes, XDIM)

    own = pltpu.make_async_copy(w_ref, weight_buf.at[rank], own_sem)
    own.start()
    loads = [pltpu.make_async_copy(source, target, load_sem.at[i]) for i, (source, target) in enumerate(
        ((dup_in, dup_ref), (rup_in, rup_ref), (k_in, k_ref), (q_in, q_ref), (v_in, v_ref)))]
    for load in loads:
        load.start()

    barrier = pltpu.get_barrier_semaphore()

    @pl.loop(1, devices)
    def _(j):
        pl.semaphore_signal(barrier, inc=1, device_id={"sp": lax.rem(me + j, devices)}, device_id_type=MESH)

    for target in (at_rank(along(1)), at_rank(along(-1)), mate):
        pl.semaphore_signal(barrier, inc=1, device_id=target, device_id_type=MESH)

    last = 2 * half_way - 2

    def quarters(source, kind, start):
        return weight_buf.at[source * 2 + kind, pl.ds(pl.multiple_of(start, quarter), quarter)]

    def remote(ref, sem_out, sem_in, target):
        return pltpu.make_async_remote_copy(
            src_ref=ref, dst_ref=ref, send_sem=sem_out, recv_sem=sem_in, device_id=target, device_id_type=MESH)

    def turn(way):
        return 1 if way == 0 else -1

    def part_of(n, way):
        half = lax.rem(n, 2)
        return half if way == 0 else 1 - half

    def ring(n, way, hops):
        source = along(-turn(way) * hops)
        ref = quarters(source, core, parity * rows + part_of(n, way) * quarter)
        return remote(ref, sent_ring_sem.at[way, n], ring_sem.at[way, n], at_rank(along(turn(way))))

    def ring_out(n, way):
        return ring(n, way, n // 2)

    def ring_in(n, way):
        return ring(n, way, n // 2 + 1)

    def cross(n, way, own_side):
        part = part_of(n, way)
        side = parity if own_side else 1 - parity
        ref = quarters(along(-turn(way) * (n // 2 + 1)), core, side * rows + part * quarter)
        return remote(ref, sent_cross_sem.at[way, n], cross_sem.at[way, n], across(1 - 2 * part))

    def to_mate(n, way, own_side, kind):
        side = parity if own_side else 1 - parity
        ref = quarters(along(-turn(way) * (n // 2 + 1)), kind, side * rows + part_of(n, way) * quarter)
        which = 0 if own_side else 1
        return remote(ref, sent_mate_sem.at[way, which, n], mate_sem.at[way, which, n], mate)

    def whole_to_mate(kind):
        return remote(weight_buf.at[line * 2 + kind], sent_whole_sem, whole_sem, mate)

    def serve_ring(n):
        for way in range(2):
            ring_in(n, way).wait_recv()

            @pl.when(n + 2 <= last)
            def _():
                ring_out(n + 2, way).start()

        for way in range(2):
            cross(n, way, True).start()
            to_mate(n, way, True, core).start()

    def serve_cross(n):
        for way in range(2):
            cross(n, way, False).wait_recv()
            to_mate(n, way, False, core).start()

    pl.semaphore_wait(barrier, devices - 1 + 3)
    own.wait()
    for n in range(2 if half_way > 1 else 1):
        for way in range(2):
            ring_out(n, way).start()
    whole_to_mate(core).start()

    rounds = pairs // batch

    def serve(n):
        @pl.when(n <= last)
        def _():
            serve_ring(n)

            @pl.when(n >= 2)
            def _():
                serve_cross(n - 2)

    for load in loads:
        load.wait()
    squashed = jnp.tanh(low_ref[...].astype(F32)).astype(BF16)
    rate_low = rate_ref[...]

    @pl.loop(0, rounds)
    def _(b):
        wavefront([prepare(size, pl.ds(pl.multiple_of((b * (batch // 2) + i) * QUAD, QUAD), QUAD), q_ref, k_ref,
                           squashed, rate_low, dup_ref, rup_ref, base_ref, ops, decay_buf,
                           2 * (b * (batch // 2) + i)) for i in range(batch // 2)])

    def head_copy(head, sender, target):
        return pltpu.make_async_remote_copy(
            src_ref=message_buf.at[head], dst_ref=arrive_buf.at[sender], send_sem=sent_sem, recv_sem=message_sem,
            device_id=target, device_id_type=MESH)

    def decay_copy(head, sender, target):
        return pltpu.make_async_remote_copy(
            src_ref=decay_buf.at[head], dst_ref=arrive_decay.at[sender], send_sem=sent_decay_sem,
            recv_sem=decay_sem, device_id=target, device_id_type=MESH)

    @pl.loop(0, pairs // batch)
    def _(b):
        ats = [pl.ds(pl.multiple_of((b * batch + i) * PAIR, PAIR), PAIR) for i in range(batch)]
        messages = transitions(size, ats, v_ref, ops, solved_bufs, lambda: serve(2 * b))
        for i, (first, second) in enumerate(messages):
            message_buf[2 * (b * batch + i)] = first
            message_buf[2 * (b * batch + i) + 1] = second
        count = 2 * batch

        @pl.loop(0, count)
        def _(j):
            head = b * count + lax.rem(me + j, count)

            @pl.when(head != my_head)
            def _():
                head_copy(head, me, {"sp": keeper(head)}).start()
                decay_copy(head, me, {"sp": keeper(head)}).start()

        serve(2 * b + 1)

    arrive_buf[me] = message_buf[my_head]
    arrive_decay[me] = decay_buf[my_head]
    @pl.loop(0, pairs // batch)
    def _(b):
        wavefront([readouts(size, pl.ds(pl.multiple_of((b * batch + i) * PAIR, PAIR), PAIR), v_ref, ops,
                            solved_bufs, local_bufs) for i in range(batch)])
        serve(2 * rounds + b)

    seen = min(3 * rounds, last + 1)
    for n in range(seen, last + 1):
        serve_ring(n)
    others = pl.ds(0, devices - 1)
    pltpu.make_async_copy(arrive_buf.at[others], arrive_buf.at[others], message_sem).wait()
    pltpu.make_async_copy(arrive_decay.at[others], arrive_decay.at[others], decay_sem).wait()

    def back_copy(chunk, head, target):
        return pltpu.make_async_remote_copy(
            src_ref=back_buf.at[chunk], dst_ref=start_buf.at[head], send_sem=sent_back_sem, recv_sem=back_sem.at[head],
            device_id=target, device_id_type=MESH)

    row = iota((HEAD, PAIR), 0)
    lane = iota((HEAD, PAIR), 1)
    lower = lane < HEAD
    marker = jnp.where(lane == row + HEAD, F32(1.0), F32(0.0)).astype(BF16)
    marker = cat([jnp.zeros_like(marker), marker], 0)
    low_tall = iota((PAIR, PAIR), 1) < HEAD
    begin = jnp.where(iota((PAIR, PAIR), 0) == iota((PAIR, PAIR), 1), F32(1.0), F32(0.0))
    begin = jnp.where(low_tall, begin, 0.0)
    per = devices // XDIM
    steps = [[begin] for _ in range(XDIM)]
    for r in range(per):
        for g in range(XDIM):
            if g == XDIM - 1 and r == per - 1:
                continue
            c = g * per + r
            now = steps[g][-1]
            message = arrive_buf[c]
            moved = mm_nt(jnp.where(low_tall, now.astype(BF16), marker), cat([message, jnp.zeros_like(message)], 0))
            steps[g].append(moved + now * arrive_decay[c])

    def put_back(c, state):
        average = jnp.mean(state, axis=0, keepdims=True)
        centred = jnp.where(lower, state - average, 0.0)
        back_buf[c] = (centred[: HEAD // 2] + pltpu.roll(centred[HEAD // 2 :], HEAD, 1)).astype(BF16)

    state = jnp.zeros((HEAD, PAIR), F32)
    for g in range(XDIM):
        high, low = split(state)
        left = cat([jnp.where(lower, high, jnp.zeros_like(high)), jnp.where(lower, low, jnp.zeros_like(low))], 0)
        for r in range(per + 1):
            if g == XDIM - 1 and r == per:
                continue
            both = steps[g][r]
            if r == 0:
                reached = state
            elif g == 0:
                reached = both[HEAD:]
            else:
                moved = mm(left, both.astype(BF16))
                reached = moved[:HEAD] + moved[HEAD:] + both[HEAD:]
            if r < per:
                put_back(g * per + r, reached)
            else:
                state = reached

    @pl.loop(1, devices)
    def _(j):
        chunk = lax.rem(me + j, devices)
        back_copy(chunk, my_head, {"sp": chunk}).start()

    start_buf[my_head] = back_buf[me]

    for n in range(max(seen - 2, 0), last + 1):
        serve_cross(n)

    mean_ones = cat([same_head_ones(PAIR, 1.0 / HEAD)] * 2, 0)
    centring = jnp.where(lane == row + HEAD, F32(1.0 - 1.0 / HEAD), F32(-1.0 / HEAD)).astype(BF16)

    def finish_wait(p):
        for i in range(2):
            head = 2 * p + i

            @pl.when(head != my_head)
            def _():
                back_copy(me, head, {"sp": me}).wait_recv()

    def finish_pair(p):
        at = pl.ds(pl.multiple_of(p * PAIR, PAIR), PAIR)
        wide = pl.ds(pl.multiple_of(p * QUAD, QUAD), QUAD)
        rights = []
        for i in range(2):
            packed = start_buf[2 * p + i]
            rights.append(jnp.where(lower, cat([packed, swap_halves(packed)], 0), centring))
        right = diag2(rights[0], rights[1])
        centred = mm_nt(local_high[:, wide], right) + mm_nt(local_low[:, wide], right)
        yield
        variance = mm(cat(split(centred * centred), 1), mean_ones)
        yield
        mix_buf[:, at] = (centred * lax.rsqrt(variance + 1.0) * gain_ref[:, at]).astype(BF16)

    @pl.loop(0, pairs // batch)
    def _(b):
        for i in range(batch):
            finish_wait(b * batch + i)
        wavefront([finish_pair(b * batch + i) for i in range(batch)])

    def project(offset):
        at = along(offset)
        weight = cat([weight_buf[2 * at], weight_buf[2 * at + 1]], 1)
        out_ref[:, pl.ds(pl.multiple_of(at * QUAD, QUAD), QUAD)] = mm(mix_buf[...], weight).astype(BF16)

    whole_to_mate(1 - core).wait_recv()
    project(0)
    for n in range(last + 1):
        for way in range(2):
            for own_side in (True, False):
                to_mate(n, way, own_side, 1 - core).wait_recv()
    for offset in [o for step in range(1, half_way) for o in (-step, step)] + [half_way]:
        project(offset)

    pltpu.make_async_copy(message_buf.at[others], message_buf.at[others], sent_sem).wait()
    pltpu.make_async_copy(decay_buf.at[others], decay_buf.at[others], sent_decay_sem).wait()
    pltpu.make_async_copy(back_buf.at[others], back_buf.at[others], sent_back_sem).wait()
    whole_to_mate(core).wait_send()

    @pl.loop(0, last + 1)
    def _(n):
        for way in range(2):
            ring_out(n, way).wait_send()
            for own_side in (True, False):
                to_mate(n, way, own_side, core).wait_send()
            cross(n, way, True).wait_send()


def per_device(devices, ranks, query_rows, key_rows, value_rows, decay_low, rate_low, decay_up, rate_up,
               decay_base, norm_gain, out_weight):
    size, width = query_rows.shape[1:]
    heads = width // HEAD
    batch = min(8, width // PAIR)
    length = ranks // 2
    pieces = 2 * (length // 2) - 1
    anywhere = pl.BlockSpec(memory_space=pl.ANY)
    vmem = pl.BlockSpec(memory_space=pltpu.VMEM)
    dma = pltpu.SemaphoreType.DMA
    wide = lambda lanes: pltpu.VMEM((size, lanes), BF16)
    out = pl.pallas_call(
        functools.partial(mixer_kernel, devices, ranks, batch),
        in_specs=[anywhere] * 3 + [vmem] * 2 + [anywhere] * 2 + [vmem] * 2 + [anywhere],
        out_specs=vmem,
        out_shape=jax.ShapeDtypeStruct((size, out_weight.shape[1] * ranks), BF16),
        scratch_shapes=[wide(width)] * 3 + [pltpu.VMEM(decay_up.shape, BF16)] * 2 + [dma((5,))]
        + [wide(width) for _ in range(10)] + [pltpu.VMEM((size, width), F32)] * 2
        + [wide(2 * width) for _ in range(4)] + [wide(width)] + [
            pltpu.VMEM((heads, HEAD, PAIR), BF16),
            pltpu.VMEM((heads, 1, PAIR), F32),
            pltpu.VMEM((devices, HEAD, PAIR), BF16),
            pltpu.VMEM((devices, 1, PAIR), F32),
            pltpu.VMEM((devices, HEAD // 2, PAIR), BF16),
            pltpu.VMEM((heads, HEAD // 2, PAIR), BF16),
            pltpu.VMEM((ranks,) + out_weight.shape, BF16),
            dma, dma, dma((heads,)), dma, dma, dma,
            dma((2, pieces)), dma((2, pieces)), dma((2, 2, pieces)), dma,
            dma((2, pieces)), dma((2, pieces)), dma((2, 2, pieces)), dma, dma,
        ],
        compiler_params=pltpu.CompilerParams(
            collective_id=0, has_side_effects=True, vmem_limit_bytes=60 * 2**20),
        cost_estimate=pl.CostEstimate(flops=10**10, bytes_accessed=10**7, transcendentals=0),
        name="mixer",
    )(query_rows[0], key_rows[0], value_rows[0], decay_low[0], rate_low[0], decay_up, rate_up,
      decay_base[None], norm_gain[None], out_weight)
    return out[None]


def solution(mesh):
    in_specs = (
        P("dp", "sp", None),
        P("dp", "sp", None),
        P("dp", "sp", None),
        P("dp", "sp", None),
        P("dp", "sp", None),
        P(),
        P(),
        P(),
        P(),
        P(None, "dp"),
    )
    return jax.shard_map(
        functools.partial(per_device, mesh.shape["sp"], mesh.shape["dp"]),
        mesh=mesh, in_specs=in_specs, out_specs=P("dp", "sp", None), check_vma=False,
    )
```
